512 devices in a mesh: ep: 32 (over z, core), tp: 16 (over y, x).
Axes of the slice: x: 4, y: 4, z: 16, core: 2. Of those that a mesh axis runs over, the one named last changes fastest.
Arguments:
- branch_in: bfloat16 [131072, 512], P(('ep', 'tp')), may hold values from -6 to 6
- pool_weight: bfloat16 [4, 128, 128], replicated, may hold values from -0.5 to 0.5
- group_gain: float32 [512], replicated, may hold values from 0.1 to 1.9
- out_weight: bfloat16 [512, 2048], P(None, 'tp'), may hold values from -0.25 to 0.25
- out_gain: float32 [2048], replicated, may hold values from 0.1 to 1.9
- ffn_input: bfloat16 [4096, 2048], P('ep'), may hold values from -6 to 6
- ffn_gain: float32 [2048], replicated, may hold values from 0.1 to 1.9
- routes: int32 [4096, 4], P('ep'), may hold values from 0 to 31, all different within a row; in each aligned block of 128 rows (0 to 127, 128 to 255, ...) at most 32 rows name the same one
- route_weight: float32 [4096, 4], P('ep'), may hold values from 0.2 to 2
- gate_weight: bfloat16 [32, 2048, 4096], P('ep', None, 'tp'), may hold values from -0.375 to 0.375
- up_weight: bfloat16 [32, 2048, 4096], P('ep', None, 'tp'), may hold values from -0.375 to 0.375
- down_weight: bfloat16 [32, 4096, 2048], P('ep', 'tp'), may hold values from -0.0078125 to 0.0078125
Outputs:
- mixer_out: bfloat16 [131072, 2048], P(('ep', 'tp'))
- expert_out: bfloat16 [4096, 2048], P('ep', 'tp')
The draws below stay inside these ranges and needn't reach their ends.
Inputs may be any that keep to these rules, and one draw needn't show every extreme that they name: `routes`: each row names 4 different experts. Among the 128 rows of one index of ep no expert is named by more than 32 rows, and in some such block one expert is named by exactly 32.
All inputs are finite; a program needn't handle non-finite values.
Results may differ from the reference program's by a relative error of at most 0.017.
Values may be sent and summed in bfloat16 or wider, within the bound.
A program may use at most 64 MiB of HBM per device.

```python
import math
import jax
import jax.numpy as jnp
import numpy as np
from jax import lax

D = 2048
POOL_CH = 128
GW = 512
FF = 4096
TOPK = 4
RA = 256
RB = 128
EXPERTS = 32
CAP = 32
TOKENS_A = 131072
TOKENS_B = 4096
N_EP = 32
N_TP = 16


def block_scale(rng, dims, split, least, largest):
    level = 1.0
    for axis_at, blocks in split:
        draws = jax.random.uniform(jax.random.fold_in(jax.random.fold_in(rng, 6), axis_at), (blocks,), jnp.float32, least / len(split), largest / len(split))
        level = level * jnp.repeat(jnp.exp(draws), dims[axis_at] // blocks).reshape((-1,) + (1,) * (len(dims) - 1 - axis_at))
    return level


def routed_block(stream_key, own, number, rows, amount, top, most, lean):
    ranking = jax.random.permutation(stream_key, amount)
    heavy_load, usual = shares(amount, rows * top, most, lean, True), shares(amount, rows * top, most, lean, False)
    places = jnp.arange(amount)

    def named(lengths, rotation):
        used = int((lengths > 0).sum())
        fixed = max(1, used // 4)
        passed = fixed + (places - fixed + rotation * (used - fixed)) % max(1, amount - fixed)
        return jnp.zeros((amount,), jnp.int32).at[ranking[jnp.where(places < fixed, places, passed)]].set(jnp.asarray(lengths, jnp.int32))

    lengths = jnp.where(number % 4 == 0, named(heavy_load, number // 4), named(usual, number - number // 4 - 1))
    mixed = jax.random.permutation(jax.random.fold_in(own, 3), amount)
    source_of, receiver = mixed[0:amount // 2 * 2:2], mixed[1:amount // 2 * 2:2]
    room = jnp.minimum(lengths[source_of] - 1, most - lengths[receiver]) // 2
    room = jnp.where((source_of == ranking[0]) | (receiver == ranking[0]) | (lengths[receiver] == 0), 0, jnp.maximum(room, 0))
    passed = jax.random.randint(jax.random.fold_in(own, 4), (amount // 2,), 0, 1 << 20) % (room + 1)
    lengths = lengths.at[source_of].add(-passed).at[receiver].add(passed)
    labels = jnp.searchsorted(jnp.cumsum(lengths), jnp.arange(rows * top), side="right").astype(jnp.int32)
    listing = labels.reshape(top, rows).T
    listing = listing[jax.random.permutation(jax.random.fold_in(own, 1), rows)]
    rotation = jax.random.randint(jax.random.fold_in(own, 2), (rows, 1), 0, top)
    return jnp.take_along_axis(listing, (jnp.arange(top)[None, :] + rotation) % top, axis=1)


def shares(number_of, total, limit, skew, full):
    loads = [(1 << 20) // math.isqrt(standing ** skew) + 1 for standing in range(1, number_of + 1)]
    largest = limit if full else min(limit, max(-(-total // number_of), total * loads[0] // sum(loads)))
    least = 1 if total - largest >= number_of - 1 else 0
    holding, rest = [largest] + [least] * (number_of - 1), total - largest - least * (number_of - 1)
    while rest > 0:
        candidates = [i for i in range(1, number_of) if holding[i] < largest] or [i for i in range(1, number_of) if holding[i] < limit]
        pool, remaining = sum([loads[i] for i in candidates]), rest
        for i in candidates:
            addition = min(limit - holding[i], max(1, remaining * loads[i] // pool), rest)
            holding[i] = holding[i] + addition
            rest = rest - addition
    return np.array(holding)


def scatter_about(stream_key, dims, spread, limit, pieces=(), held_as=jnp.bfloat16):
    result = jax.random.normal(stream_key, dims, jnp.float32) * spread
    if len(pieces) > 0:
        result = block_scale(stream_key, dims, pieces, -0.22, 0.18) * result
    return jnp.clip(result, min=-limit, max=limit).astype(held_as)


def setup_inputs(seed: int = 0) -> dict:
    keys = jax.random.split(jax.random.key(seed), 13)
    branch_in = scatter_about(keys[0], (TOKENS_A, GW), 1.0, 6.0, ((0, 512),))
    pool_weight = scatter_about(keys[1], (4, POOL_CH, POOL_CH), POOL_CH ** -0.5, 0.5)
    group_gain = jnp.clip(1.0 + 0.18 * jax.random.normal(keys[2], (GW,), jnp.float32), 0.1, 1.9)
    out_weight = scatter_about(keys[3], (GW, D), GW ** -0.5, 0.25, ((1, 16),))
    out_gain = jnp.clip(1.0 + 0.18 * jax.random.normal(keys[4], (D,), jnp.float32), 0.1, 1.9)
    ffn_input = scatter_about(keys[5], (TOKENS_B, D), 1.0, 6.0, ((0, 32),))
    ffn_gain = jnp.clip(1.0 + 0.18 * jax.random.normal(keys[6], (D,), jnp.float32), 0.1, 1.9)
    routes_keys = jax.random.split(jax.random.fold_in(keys[7], 1), TOKENS_B // RB)
    routes_turns = jax.random.permutation(jax.random.fold_in(keys[7], 3), TOKENS_B // RB)
    routes = jax.vmap(lambda own, number: routed_block(jax.random.fold_in(keys[7], 2), own, number, RB, EXPERTS, TOPK, CAP, 2))(routes_keys, routes_turns).reshape((TOKENS_B, TOPK))
    route_weight = jnp.clip(jnp.exp(math.log(2.0) - 2.3025851 * jax.random.uniform(keys[8], (TOKENS_B, TOPK), jnp.float32) ** block_scale(keys[8], (TOKENS_B, TOPK), ((0, 32),), -0.2, 0.2)), 0.2, 2.0)
    gate_weight = scatter_about(keys[9], (EXPERTS, D, FF), (D // 9) ** -0.5, 0.375, ((0, 32), (2, 16)))
    up_weight = scatter_about(keys[10], (EXPERTS, D, FF), (D // 9) ** -0.5, 0.375, ((0, 32), (2, 16)))
    down_weight = scatter_about(keys[11], (EXPERTS, FF, D), (FF * 160) ** -0.5, 0.0078125, ((0, 32), (1, 16)))
    return dict(branch_in=branch_in, pool_weight=pool_weight, group_gain=group_gain, out_weight=out_weight, out_gain=out_gain, ffn_input=ffn_input, ffn_gain=ffn_gain, routes=routes, route_weight=route_weight, gate_weight=gate_weight, up_weight=up_weight, down_weight=down_weight)


pool_windows = (2, 4, 8, 16)
rim_rows = 15
norm_eps = 1e-06
clamp_limit = 7.0
sigmoid_slope = 1.702

def rms_scale(values, gain):
    return values * lax.rsqrt(lax.optimization_barrier(jnp.mean(values * values, axis=-1, keepdims=True)) + norm_eps) * gain.astype(jnp.float32)

def slot_tables(route_block, expert_count, capacity):
    row_count, top_count = route_block.shape
    flat_experts = route_block.reshape(-1)
    one_hot = (flat_experts[:, None] == jnp.arange(expert_count, dtype=jnp.int32)[None, :]).astype(jnp.int32)
    earlier = jnp.cumsum(one_hot, axis=0) - one_hot
    slot_index = lax.optimization_barrier(jnp.sum(earlier * one_hot, axis=1))
    flat_slots = (slot_index * expert_count + flat_experts).astype(jnp.int32)
    owner_rows = jnp.full((capacity * expert_count,), row_count, jnp.int32)
    owner_rows = owner_rows.at[flat_slots].set(jnp.arange(row_count * top_count, dtype=jnp.int32) // top_count)
    return (flat_slots, owner_rows)

def pool_reference(branch_in, pool_weight, group_gain, out_weight, out_gain):
    total_rows, width = branch_in.shape
    group_chans = width // len(pool_windows)
    widened = jnp.concatenate([jnp.zeros((rim_rows, width), jnp.bfloat16), branch_in], axis=0)
    window = jnp.repeat(jnp.array(pool_windows, jnp.int32), group_chans)

    def one_block(block_index):
        first_row = (block_index * RA).astype(jnp.int32)
        segment = lax.dynamic_slice_in_dim(widened, first_row, RA + rim_rows, 0).astype(jnp.float32)
        positions = first_row + jnp.arange(RA, dtype=jnp.int32)
        summed = jnp.zeros((RA, width), jnp.float32)
        for offset_back in range(rim_rows + 1):
            shifted = segment[rim_rows - offset_back:rim_rows - offset_back + RA]
            summed = summed + jnp.where(window[None, :] > offset_back, shifted, jnp.float32(0.0))
        counts = jnp.minimum(window[None, :], positions[:, None] + 1).astype(jnp.float32)
        pooled = (summed / counts - segment[rim_rows:]).astype(jnp.bfloat16)
        mixed_parts = []
        for group_index in range(len(pool_windows)):
            lower = group_index * group_chans
            mixed_parts.append(jnp.dot(pooled[:, lower:lower + group_chans], pool_weight[group_index], preferred_element_type=jnp.float32))
        group_mix = jnp.concatenate(mixed_parts, axis=1)
        mixed_rows = rms_scale(group_mix, group_gain).astype(jnp.bfloat16)
        projected = jnp.dot(mixed_rows, out_weight, preferred_element_type=jnp.float32)
        return rms_scale(projected, out_gain).astype(jnp.bfloat16)
    blocks = lax.map(one_block, jnp.arange(total_rows // RA, dtype=jnp.int32))
    return blocks.reshape(total_rows, out_weight.shape[1])

def expert_reference(ffn_input, ffn_gain, routes, route_weight, gate_weight, up_weight, down_weight):
    total_rows, model_width = ffn_input.shape
    top_count = routes.shape[1]
    expert_count = gate_weight.shape[0]
    hidden_width = gate_weight.shape[2]
    row_count = total_rows // N_EP
    capacity = 2 * row_count * top_count // expert_count
    normed_rows = rms_scale(ffn_input.astype(jnp.float32), ffn_gain).astype(jnp.bfloat16)
    route_blocks = routes.reshape(N_EP, row_count, top_count)
    flat_slots, owner_rows = jax.vmap(lambda route_block: slot_tables(route_block, expert_count, capacity))(route_blocks)
    padded = jnp.concatenate([normed_rows.reshape(N_EP, row_count, model_width), jnp.zeros((N_EP, 1, model_width), jnp.bfloat16)], axis=1)
    slot_rows = jax.vmap(lambda block_rows, block_owner: block_rows[block_owner])(padded, owner_rows)
    slot_rows = slot_rows.reshape(N_EP, capacity, expert_count, model_width)
    by_expert = jnp.moveaxis(slot_rows, 2, 0).reshape(expert_count, N_EP * capacity, model_width)

    def one_expert(operands):
        expert_rows, gate_local, up_local, down_local = operands
        gate_pre = jnp.minimum(jnp.dot(expert_rows, gate_local, preferred_element_type=jnp.float32), clamp_limit)
        up_pre = jnp.clip(jnp.dot(expert_rows, up_local, preferred_element_type=jnp.float32), -clamp_limit, clamp_limit)
        hidden = ((up_pre + 1.0) * gate_pre * jax.nn.sigmoid(sigmoid_slope * gate_pre)).astype(jnp.bfloat16)
        block_width = hidden_width // N_TP
        part_hidden = hidden.astype(jnp.float32).reshape(expert_rows.shape[0], N_TP, block_width)
        part_down = down_local.astype(jnp.float32).reshape(N_TP, block_width, model_width)
        partials = jnp.einsum('ntf,tfd->tnd', part_hidden, part_down)
        partials = partials.astype(jnp.bfloat16).astype(jnp.float32)
        return lax.optimization_barrier(jnp.sum(partials, axis=0)).astype(jnp.bfloat16)
    results = lax.map(one_expert, (by_expert, gate_weight, up_weight, down_weight))
    results = results.reshape(expert_count, N_EP, capacity, model_width).transpose(1, 2, 0, 3)
    results = results.reshape(N_EP, capacity * expert_count, model_width)
    picked = jax.vmap(lambda block_results, block_slots: block_results[block_slots])(results, flat_slots)
    picked = picked.reshape(total_rows, top_count, model_width).astype(jnp.float32)
    return lax.optimization_barrier(jnp.sum(picked * route_weight[:, :, None], axis=1)).astype(jnp.bfloat16)

def reference(branch_in, pool_weight, group_gain, out_weight, out_gain, ffn_input, ffn_gain, routes, route_weight, gate_weight, up_weight, down_weight):
    mixer_out = pool_reference(branch_in, pool_weight, group_gain, out_weight, out_gain)
    expert_out = expert_reference(ffn_input, ffn_gain, routes, route_weight, gate_weight, up_weight, down_weight)
    return (mixer_out, expert_out)
```

```python
import functools

import jax
import jax.numpy as jnp
from jax import lax
from jax.experimental import pallas as pl
from jax.experimental.pallas import tpu as pltpu
from jax.sharding import Mesh
from jax.sharding import PartitionSpec as P

MESH = pl.DeviceIdType.MESH
AXES = ("z", "c", "y", "x")
EP = ("z", "c")
TP = ("y", "x")

pool_windows = (2, 4, 8, 16)
norm_eps = 1e-06
clamp_limit = 7.0
sigmoid_slope = 1.702

BF = jnp.bfloat16
F32 = jnp.float32

NZ, NC, NY, NX = 16, 2, 4, 4
CAP = 32
LANE = 128
CHUNKS = 4
RIM = 16


def dot(a, b):
    return jnp.dot(a, b, preferred_element_type=F32)


def kernel(
    branch,
    pool_w,
    group_gain,
    out_w,
    out_gain,
    ffn_in,
    ffn_gain,
    routes_t,
    weight_t,
    gate_w,
    up_w,
    down_w,
    mixer_out,
    expert_out,
    full,
    other_w,
    gate_up,
    down_p,
    ext,
    mixed,
    proj,
    mixer,
    tokens,
    hot,
    picked,
    part,
    rx1,
    rx2,
    sum_x,
    ry1,
    ry2,
    home,
    result,
    ag_s,
    ag_r,
    rs_s,
    rs_r,
    z_s,
    z_r,
    back_s,
    back_r,
    own_s,
    swap_s,
    rim_s,
    load_s,
):
    z, c = lax.axis_index("z"), lax.axis_index("c")
    y, x = lax.axis_index("y"), lax.axis_index("x")
    ep = z * NC + c
    tp = y * NX + x
    rows_a = branch.shape[0]
    rows_b = ffn_in.shape[0]
    model = ffn_in.shape[1]
    hid = gate_w.shape[2]
    width = branch.shape[1]
    slots = NZ * NC * CAP
    crow = slots // CHUNKS
    half = crow // 2
    per = NZ // CHUNKS
    wide = NY * LANE

    spot = (ep * NY + y) * NX + x
    total = NZ * NC * NY * NX

    def place(index):
        return (index // (NC * NY * NX), (index // (NY * NX)) % NC, (index // NX) % NY, index % NX)

    after = place((spot + 1) % total)
    before = place((spot + total - 1) % total)
    x_to = ((z, c, y, (x + 1) % NX), (z, c, y, (x + NX - 1) % NX))
    y_to = ((z, c, (y + 1) % NY, x), (z, c, (y + NY - 1) % NY, x))
    partner = (z, 1 - c, y, x)

    def step_z(i):
        return (z + NZ + ((i + 1) // 2) * (2 * (i % 2) - 1)) % NZ

    loads = {}

    def load(name, src, dst, slot):
        copy = pltpu.make_async_copy(src, dst, load_s.at[slot])
        copy.start()
        loads[name] = copy

    load("tokens", ffn_in, tokens, 0)
    load("branch", branch, ext.at[pl.ds(RIM, rows_a)], 1)
    own_cols = pl.ds(pl.multiple_of(tp * LANE, LANE), LANE)
    load("out_w", out_w.at[pl.ds(pl.multiple_of(c * crow, crow), crow)], full.at[pl.ds(0, crow), own_cols], 2)
    load("gate", gate_w.at[0], gate_up.at[:, pl.ds(0, hid)], 3)
    load("up", up_w.at[0], gate_up.at[:, pl.ds(hid, hid)], 4)
    for a in range(NY):
        for b in range(NX):
            load(
                ("down", a, b),
                down_w.at[0, :, pl.ds((a * NX + b) * LANE, LANE)],
                down_p.at[:, pl.ds((b * NY + a) * LANE, LANE)],
                5 + a * NX + b,
            )

    barrier = pltpu.get_barrier_semaphore()

    def greet(i, carry):
        zz = step_z(i)
        for cc in range(NC):
            pl.semaphore_signal(barrier, inc=1, device_id=(zz, cc, y, x), device_id_type=MESH)
        return carry

    for peer in (*x_to, *y_to, after, before, partner):
        pl.semaphore_signal(barrier, inc=1, device_id=peer, device_id_type=MESH)
    lax.fori_loop(1, NZ, greet, 0)

    loads["tokens"].wait()
    acc = jnp.zeros((rows_b, LANE), F32)
    for k in range(model // LANE):
        v = tokens[:, k * LANE : (k + 1) * LANE].astype(F32)
        acc = acc + v * v
    scale = lax.rsqrt(jnp.sum(acc, axis=1, keepdims=True) * (1.0 / model) + norm_eps)
    normed = (tokens[:, own_cols].astype(F32) * scale * ffn_gain[:, own_cols]).astype(BF)

    experts = NZ * NC
    ids = lax.broadcasted_iota(jnp.int32, (experts, rows_b), 0)
    named = jnp.zeros((experts, rows_b), F32)
    weight = jnp.zeros((experts, rows_b), F32)
    for k in range(routes_t.shape[0]):
        hit = ids == routes_t[k : k + 1, :]
        named = named + jnp.where(hit, 1.0, 0.0)
        weight = weight + jnp.where(hit, weight_t[k : k + 1, :], 0.0)
    earlier = jnp.where(
        lax.broadcasted_iota(jnp.int32, (rows_b, rows_b), 0)
        < lax.broadcasted_iota(jnp.int32, (rows_b, rows_b), 1),
        1.0,
        0.0,
    ).astype(BF)
    place_of = jnp.where(named > 0.5, dot(named.astype(BF), earlier), -1.0)
    slot_ids = lax.broadcasted_iota(jnp.int32, (CAP, rows_b), 0).astype(F32)
    for e in range(experts):
        hot[e * CAP : (e + 1) * CAP, :] = jnp.where(slot_ids == place_of[e : e + 1, :], 1.0, 0.0).astype(BF)
    picked[...] = dot(hot[...], normed).astype(BF)

    pl.semaphore_wait(barrier, 2 * (NZ - 1) + 7)

    loads["branch"].wait()
    rim = pltpu.make_async_remote_copy(
        ext.at[pl.ds(rows_a, RIM)],
        ext.at[pl.ds(0, RIM)],
        send_sem=rim_s.at[0],
        recv_sem=rim_s.at[1],
        device_id=after,
        device_id_type=MESH,
    )
    rim.start()

    def base(g):
        return g * crow

    sends = [rim]

    def push(src, dst, sems, index, peer):
        send, recv = sems
        copy = pltpu.make_async_remote_copy(
            src,
            dst,
            send_sem=send.at[index],
            recv_sem=recv.at[index],
            device_id=peer,
            device_id_type=MESH,
        )
        copy.start()
        sends.append(copy)
        return copy

    gather = {}

    def cols_x(which):
        return pl.ds(pl.multiple_of((y * NX + which % NX) * LANE, LANE), LANE)

    def cols_y(which):
        return pl.ds(pl.multiple_of((which % NY) * wide, wide), wide)

    def ag1(g):
        ref = full.at[pl.ds(base(g), crow), cols_x(x)]
        gather[g, 0] = [push(ref, ref, (ag_s, ag_r), g * 8 + d, x_to[d]) for d in range(2)]

    def ag2(g):
        out = []
        for d in range(2):
            gather[g, 0][d].wait_recv()
            ref = full.at[pl.ds(base(g) + d * half, half), cols_x(x + NX - 1 + 2 * d)]
            out.append(push(ref, ref, (ag_s, ag_r), g * 8 + 2 + d, x_to[d]))
        gather[g, 1] = out

    def ag3(g):
        for d in range(2):
            gather[g, 1][d].wait_recv()
        ref = full.at[pl.ds(base(g), crow), cols_y(y)]
        gather[g, 2] = [push(ref, ref, (ag_s, ag_r), g * 8 + 4 + d, y_to[d]) for d in range(2)]

    def ag4(g):
        out = []
        for d in range(2):
            gather[g, 2][d].wait_recv()
            ref = full.at[pl.ds(base(g) + d * half, half), cols_y(y + NY - 1 + 2 * d)]
            out.append(push(ref, ref, (ag_s, ag_r), g * 8 + 6 + d, y_to[d]))
        gather[g, 3] = out

    def ag5(g):
        for d in range(2):
            gather[g, 3][d].wait_recv()

    own_pick = pltpu.make_async_copy(
        picked.at[pl.ds(pl.multiple_of(ep * CAP, CAP), CAP)],
        full.at[pl.ds(pl.multiple_of(crow + c * CAP, CAP), CAP), own_cols],
        own_s.at[0],
    )

    def dispatch(i, zz, cc, seat):
        row = pl.multiple_of(crow + (seat * NC + c) * CAP, CAP)
        return pltpu.make_async_remote_copy(
            picked.at[pl.ds(pl.multiple_of((zz * NC + cc) * CAP, CAP), CAP)],
            full.at[pl.ds(row, CAP), own_cols],
            send_sem=z_s.at[0],
            recv_sem=z_r.at[seat // per],
            device_id=(zz, cc, y, x),
            device_id_type=MESH,
        )

    def dispatch_all(i, carry):
        zz = step_z(i)
        seat = jnp.minimum(i + 2 * (i % 2) - 1, NZ - 1)
        for cc in range(NC):
            dispatch(i, zz, cc, seat).start()
        return carry

    loads["out_w"].wait()
    own_pick.start()
    dispatch(0, z, 1 - c, 0).start()
    ag1(0)
    lax.fori_loop(1, NZ, dispatch_all, 0)

    def arrived(g):
        count = crow - CAP if g == 1 else crow
        ref = full.at[pl.ds(base(g), count), own_cols]
        pltpu.make_async_copy(ref, ref, z_r.at[g - 1]).wait()
        if g == 1:
            own_pick.wait()

    def pool_mix():
        rim.wait_recv()
        reach = rows_a + RIM
        row = lax.broadcasted_iota(jnp.int32, (rows_a, reach), 0) + RIM
        col = lax.broadcasted_iota(jnp.int32, (rows_a, reach), 1)
        first = jnp.where(spot == 0, RIM, 0)
        age = jnp.where(col < first, reach, row - col)
        position = spot * rows_a + lax.broadcasted_iota(jnp.int32, (rows_a, LANE), 0)
        parts = []
        acc = jnp.zeros((rows_a, LANE), F32)
        for k, window in enumerate(pool_windows):
            cols = slice(k * LANE, (k + 1) * LANE)
            band = jnp.where((age >= 0) & (age < window), 1.0, 0.0).astype(BF)
            summed = dot(band, ext[:, cols])
            count = jnp.minimum(position + 1, window).astype(F32)
            pooled = (summed / count - ext[RIM:, cols].astype(F32)).astype(BF)
            mix = dot(pooled, pool_w[k])
            parts.append(mix)
            acc = acc + mix * mix
        scale = lax.rsqrt(jnp.sum(acc, axis=1, keepdims=True) * (1.0 / width) + norm_eps)
        for k, mix in enumerate(parts):
            cols = slice(k * LANE, (k + 1) * LANE)
            mixed[:, cols] = (mix * scale * group_gain[:, cols]).astype(BF)

    swap = pltpu.make_async_remote_copy(
        full.at[pl.ds(0, crow)],
        other_w,
        send_sem=swap_s.at[0],
        recv_sem=swap_s.at[1],
        device_id=partner,
        device_id_type=MESH,
    )

    def swap_halves():
        swap.start()
        sends.append(swap)

    store = pltpu.make_async_copy(mixer, mixer_out, load_s.at[21])

    def pool_out():
        swap.wait_recv()
        mine = mixed[:, pl.ds(pl.multiple_of(c * crow, crow), crow)]
        theirs = mixed[:, pl.ds(pl.multiple_of((1 - c) * crow, crow), crow)]
        acc = jnp.zeros((rows_a, LANE), F32)
        tile = 256
        for n in range(model // tile):
            cols = slice(n * tile, (n + 1) * tile)
            v = dot(mine, full[0:crow, cols]) + dot(theirs, other_w[:, cols])
            proj[:, cols] = v
            for k in range(tile // LANE):
                w = v[:, k * LANE : (k + 1) * LANE]
                acc = acc + w * w
        scale = lax.rsqrt(jnp.sum(acc, axis=1, keepdims=True) * (1.0 / model) + norm_eps)
        for n in range(model // tile):
            cols = slice(n * tile, (n + 1) * tile)
            mixer[:, cols] = (proj[:, cols] * scale * out_gain[:, cols]).astype(BF)
        store.start()

    reduce = {}

    def block(which, count):
        return pl.ds(pl.multiple_of((which % NX) * count, count), count)

    def compute(g):
        ag5(g)
        if g == 1:
            loads["gate"].wait()
            loads["up"].wait()
            for a in range(NY):
                for b in range(NX):
                    loads["down", a, b].wait()
        both = dot(full[base(g) : base(g) + crow, :], gate_up[...])
        gate = jnp.minimum(both[:, :hid], clamp_limit)
        up = jnp.clip(both[:, hid:], -clamp_limit, clamp_limit)
        hidden = ((up + 1.0) * gate * jax.nn.sigmoid(sigmoid_slope * gate)).astype(BF)
        r = base(g - 1)
        for k in range(NX):
            cols = block(x + 2 + k, wide)
            part[r : r + crow, cols] = dot(hidden, down_p[:, cols]).astype(BF)
            if k == 0:
                reduce[g, 0] = [
                    push(
                        part.at[pl.ds(r + d * half, half), cols],
                        rx1.at[pl.ds(r + d * half, half)],
                        (rs_s, rs_r),
                        (g - 1) * 8 + d,
                        x_to[d],
                    )
                    for d in range(2)
                ]

    def add(*values):
        out = values[0].astype(F32)
        for v in values[1:]:
            out = out + v.astype(F32)
        return out.astype(BF)

    def rs2(g):
        r = base(g - 1)
        out = []
        for d in range(2):
            reduce[g, 0][d].wait_recv()
            cols = block(x + 1 + 2 * d, wide)
            rows = slice(r + d * half, r + d * half + half)
            part[rows, cols] = add(part[rows, cols], rx1[rows, :])
            out.append(
                push(
                    part.at[pl.ds(r, crow), cols],
                    rx2.at[pl.ds(r, crow), pl.ds(d * wide, wide)],
                    (rs_s, rs_r),
                    (g - 1) * 8 + 2 + d,
                    x_to[d],
                )
            )
        reduce[g, 1] = out

    def rs3(g):
        r = base(g - 1)
        for d in range(2):
            reduce[g, 1][d].wait_recv()
        rows = slice(r, r + crow)
        sum_x[rows, :] = add(part[rows, block(x, wide)], rx2[rows, :wide], rx2[rows, wide:])
        cols = block(y + 2, LANE)
        reduce[g, 2] = [
            push(
                sum_x.at[pl.ds(r + d * half, half), cols],
                ry1.at[pl.ds(r + d * half, half)],
                (rs_s, rs_r),
                (g - 1) * 8 + 4 + d,
                y_to[d],
            )
            for d in range(2)
        ]

    def rs4(g):
        r = base(g - 1)
        out = []
        for d in range(2):
            reduce[g, 2][d].wait_recv()
            cols = block(y + 1 + 2 * d, LANE)
            rows = slice(r + d * half, r + d * half + half)
            sum_x[rows, cols] = add(sum_x[rows, cols], ry1[rows, :])
            out.append(
                push(
                    sum_x.at[pl.ds(r, crow), cols],
                    ry2.at[pl.ds(r, crow), pl.ds(d * LANE, LANE)],
                    (rs_s, rs_r),
                    (g - 1) * 8 + 6 + d,
                    y_to[d],
                )
            )
        reduce[g, 3] = out

    own_rows = pl.ds(pl.multiple_of(ep * CAP, CAP), CAP)
    own_back = pltpu.make_async_copy(
        home.at[pl.ds(pl.multiple_of(c * CAP, CAP), CAP)], result.at[own_rows], own_s.at[1]
    )

    def give_back(i, cc):
        return pltpu.make_async_remote_copy(
            home.at[pl.ds(pl.multiple_of((i * NC + cc) * CAP, CAP), CAP)],
            result.at[own_rows],
            send_sem=back_s.at[0],
            recv_sem=back_r.at[0],
            device_id=(step_z(i), cc, y, x),
            device_id_type=MESH,
        )

    def rs5(g):
        r = base(g - 1)
        for d in range(2):
            reduce[g, 3][d].wait_recv()
        rows = slice(r, r + crow)
        home[rows, :] = add(sum_x[rows, block(y, LANE)], ry2[rows, :LANE], ry2[rows, LANE:])
        low = (g - 1) * per
        if g == 1:
            own_back.start()
            give_back(0, 1 - c).start()
            low = 1

        def one(i, carry):
            for cc in range(NC):
                give_back(i, cc).start()
            return carry

        lax.fori_loop(low, g * per, one, 0)

    stages = (ag1, ag2, ag3, ag4, compute, rs2, rs3, rs4, rs5)
    for tick in range(len(stages) + CHUNKS):
        for g in range(CHUNKS + 1):
            k = tick - g
            if g == 0:
                if 1 <= k < 4:
                    stages[k](0)
                elif k == 4:
                    ag5(0)
                    swap_halves()
            elif 0 <= k < len(stages):
                if k == 0:
                    if g == 1:
                        pool_mix()
                    arrived(g)
                stages[k](g)
        if tick == 7:
            pool_out()

    own_back.wait()
    ref = result.at[pl.ds(0, slots - CAP)]
    pltpu.make_async_copy(ref, ref, back_r.at[0]).wait()
    ref = picked.at[pl.ds(0, slots - CAP)]
    pltpu.make_async_copy(ref, ref, z_s.at[0]).wait()
    w_hi = weight.astype(BF).astype(F32)
    w_lo = weight - w_hi
    acc = jnp.zeros((rows_b, LANE), F32)
    for e in range(experts):
        rows = slice(e * CAP, (e + 1) * CAP)
        h = hot[rows, :].astype(F32)
        picked[rows, :] = (h * w_hi[e : e + 1, :]).astype(BF)
        hot[rows, :] = (h * w_lo[e : e + 1, :]).astype(BF)
    over = (((0,), (0,)), ((), ()))
    value = lax.dot_general(picked[...], result[...], over, preferred_element_type=F32)
    value = value + lax.dot_general(hot[...], result[...], over, preferred_element_type=F32)
    expert_out[...] = value.astype(BF)

    store.wait()
    for copy in sends:
        copy.wait_send()
    ref = home.at[pl.ds(0, slots - CAP)]
    pltpu.make_async_copy(ref, ref, back_s.at[0]).wait()


def per_device(
    branch_in,
    pool_weight,
    group_gain,
    out_weight,
    out_gain,
    ffn_input,
    ffn_gain,
    routes,
    route_weight,
    gate_weight,
    up_weight,
    down_weight,
):
    rows_a, width = branch_in.shape
    rows_b, model = ffn_input.shape
    hid = gate_weight.shape[2]
    slots = NZ * NC * CAP
    crow = slots // CHUNKS
    half = crow // 2
    wide = NY * LANE
    any_ = pl.BlockSpec(memory_space=pl.ANY)
    vmem = pl.BlockSpec(memory_space=pltpu.VMEM)
    dma = pltpu.SemaphoreType.DMA
    return pl.pallas_call(
        kernel,
        name="mixer_and_experts",
        out_shape=(
            jax.ShapeDtypeStruct((rows_a, model), BF),
            jax.ShapeDtypeStruct((rows_b, LANE), BF),
        ),
        in_specs=[any_, vmem, vmem, any_, vmem, any_, vmem, vmem, vmem, any_, any_, any_],
        out_specs=(any_, vmem),
        scratch_shapes=[
            pltpu.VMEM((crow + slots, model), BF),
            pltpu.VMEM((crow, model), BF),
            pltpu.VMEM((model, 2 * hid), BF),
            pltpu.VMEM((hid, model), BF),
            pltpu.VMEM((rows_a + RIM, width), BF),
            pltpu.VMEM((rows_a, width), BF),
            pltpu.VMEM((rows_a, model), F32),
            pltpu.VMEM((rows_a, model), BF),
            pltpu.VMEM((rows_b, model), BF),
            pltpu.VMEM((slots, rows_b), BF),
            pltpu.VMEM((slots, LANE), BF),
            pltpu.VMEM((slots, model), BF),
            pltpu.VMEM((slots, wide), BF),
            pltpu.VMEM((slots, 2 * wide), BF),
            pltpu.VMEM((slots, wide), BF),
            pltpu.VMEM((slots, LANE), BF),
            pltpu.VMEM((slots, 2 * LANE), BF),
            pltpu.VMEM((slots, LANE), BF),
            pltpu.VMEM((slots, LANE), BF),
            dma(((CHUNKS + 1) * 8,)),
            dma(((CHUNKS + 1) * 8,)),
            dma((CHUNKS * 8,)),
            dma((CHUNKS * 8,)),
            dma((1,)),
            dma((CHUNKS,)),
            dma((1,)),
            dma((1,)),
            dma((2,)),
            dma((2,)),
            dma((2,)),
            dma((22,)),
        ],
        compiler_params=pltpu.CompilerParams(collective_id=0, has_side_effects=True),
    )(
        branch_in,
        pool_weight,
        group_gain[None],
        out_weight,
        out_gain[None],
        ffn_input,
        ffn_gain[None],
        routes.T,
        route_weight.T,
        gate_weight,
        up_weight,
        down_weight,
    )


def solution(mesh):
    split = Mesh(mesh.devices.reshape(NZ, NC, NY, NX), AXES)
    in_specs = (
        P(AXES, None),
        P(),
        P(),
        P(None, TP),
        P(),
        P(EP, None),
        P(),
        P(EP, None),
        P(EP, None),
        P(EP, None, TP),
        P(EP, None, TP),
        P(EP, TP, None),
    )
    out_specs = (P(AXES, None), P(EP, TP))
    return jax.shard_map(
        per_device, mesh=split, in_specs=in_specs, out_specs=out_specs, check_vma=False
    )
```

```python
import functools

import jax
import jax.numpy as jnp
from jax import lax
from jax.experimental import pallas as pl
from jax.experimental.pallas import tpu as pltpu
from jax.sharding import Mesh
from jax.sharding import PartitionSpec as P

MESH = pl.DeviceIdType.MESH
AXES = ("z", "c", "y", "x")
EP = ("z", "c")
TP = ("y", "x")

pool_windows = (2, 4, 8, 16)
norm_eps = 1e-06
clamp_limit = 7.0
sigmoid_slope = 1.702

BF = jnp.bfloat16
F32 = jnp.float32

NZ, NC, NY, NX = 16, 2, 4, 4
CAP = 32
LANE = 128
CHUNKS = 8
NEAR = 5
RIM = 16
WZ = 4
BACK = 1
ORDER = (
    ("w1",), ("w2",), ("ag1", 0), ("w3",), ("ag1", 1), ("ag2", 0, 0), ("ag2", 0, 1), ("ag1", 2), ("w4",),
    ("ag1", 3), ("ag3", 0), ("ag2", 1, 0), ("ag2", 1, 1), ("ag2", 2, 0), ("ag2", 2, 1), ("ag1", 4), ("w5",),
    ("ag2", 3, 0), ("ag2", 3, 1), ("ag3", 2), ("ag2", 4, 0), ("ag2", 4, 1), ("ag1", 5), ("ag1", 6),
    ("ag1", 7), ("pm",), ("ag3", 1), ("ag3", 4), ("ag4", 0, 0), ("ag4", 0, 1), ("ag3", 3), ("ag2", 6, 0),
    ("ag2", 6, 1), ("ag4", 2, 0), ("ag4", 2, 1), ("w6",), ("ag2", 5, 0), ("ag2", 5, 1), ("ag2", 7, 0),
    ("ag2", 7, 1), ("ag4", 1, 0), ("ag4", 1, 1), ("ag4", 4, 0), ("ag4", 4, 1), ("ag4", 3, 0), ("ag4", 3, 1),
    ("ag3", 6), ("w7",), ("c1", 0), ("c2", 0), ("c1", 1), ("ag3", 5), ("ag3", 7), ("c2", 1), ("c1", 2),
    ("c2", 2), ("c1", 3), ("c2", 3), ("rs2", 1, 0), ("rs2", 1, 1), ("c1", 4), ("ag4", 6, 0), ("ag4", 6, 1),
    ("c2", 4), ("po",), ("wh",), ("rs2", 0, 0), ("rs2", 0, 1), ("ag4", 5, 0), ("ag4", 5, 1), ("rs2", 2, 0),
    ("rs2", 2, 1), ("rs2", 4, 0), ("rs2", 4, 1), ("ag4", 7, 0), ("ag4", 7, 1), ("c1", 6), ("rs2", 3, 0),
    ("rs2", 3, 1), ("c2", 6), ("rs3", 0), ("rs3", 1), ("c1", 5), ("rs3", 2), ("c2", 5), ("c1", 7),
    ("c2", 7), ("rs3", 4), ("rs3", 3), ("rs4", 0, 0), ("rs4", 0, 1), ("rs2", 6, 0), ("rs2", 6, 1),
    ("rs4", 1, 0), ("rs4", 1, 1), ("rs2", 5, 0), ("rs2", 5, 1), ("rs4", 2, 0), ("rs4", 2, 1), ("rs4", 3, 0),
    ("rs4", 3, 1), ("rs2", 7, 0), ("rs2", 7, 1), ("rs4", 4, 0), ("rs4", 4, 1), ("rs5", 0), ("rs3", 6),
    ("rs5", 1), ("rs5", 3), ("rs3", 5), ("rs5", 2), ("rs4", 5, 0), ("rs4", 5, 1), ("rs3", 7), ("rs5", 4),
    ("rs4", 6, 0), ("rs4", 6, 1), ("rs5", 5), ("rs4", 7, 0), ("rs4", 7, 1), ("rs5", 6), ("rs5", 7),
)


def dot(a, b):
    return jnp.dot(a, b, preferred_element_type=F32)


def kernel(
    branch,
    pool_w_h,
    group_gain_h,
    out_w,
    out_gain_h,
    ffn_in,
    ffn_gain_h,
    routes_h,
    weight_h,
    gate_w,
    up_w,
    down_w,
    mixer_out,
    expert_out,
    pool_w,
    group_gain,
    out_gain,
    ffn_gain,
    routes_t,
    weight_t,
    full,
    full_w,
    gate_up,
    down,
    ext,
    mixed,
    proj,
    mixer,
    tokens,
    hot,
    picked,
    part,
    rx1,
    rx2,
    sum_x,
    ry1,
    ry2,
    home,
    result,
    answer,
    hidden,
    w_hi,
    w_lo,
    ag_s,
    ag_r,
    rs_s,
    rs_r,
    w_s,
    w_r,
    z_s,
    z_r,
    back_s,
    back_r,
    own_s,
    rim_s,
    load_s,
):
    z, c = lax.axis_index("z"), lax.axis_index("c")
    y, x = lax.axis_index("y"), lax.axis_index("x")
    ep = z * NC + c
    tp = y * NX + x
    tp_p = x * NY + y
    rows_a = branch.shape[0]
    rows_b = ffn_in.shape[0]
    model = ffn_in.shape[1]
    hid = gate_w.shape[2]
    width = branch.shape[1]
    slots = NZ * NC * CAP
    crow = slots // CHUNKS
    half = crow // 2
    per = NZ // CHUNKS
    wide = NY * LANE
    wrow = width // (NC * WZ)

    spot = (ep * NY + y) * NX + x
    total = NZ * NC * NY * NX

    def place(index):
        return (index // (NC * NY * NX), (index // (NY * NX)) % NC, (index // NX) % NY, index % NX)

    after = place((spot + 1) % total)
    before = place((spot + total - 1) % total)
    x_to = ((z, c, y, (x + 1) % NX), (z, c, y, (x + NX - 1) % NX))
    y_to = ((z, c, (y + 1) % NY, x), (z, c, (y + NY - 1) % NY, x))
    z_to = (((z + 1) % NZ, c, y, x), ((z + NZ - 1) % NZ, c, y, x))
    partner = (z, 1 - c, y, x)
    axis_x = (x, x_to)
    axis_y = (y, y_to)

    def order(g):
        return (axis_x, axis_y) if g % 2 == 0 else (axis_y, axis_x)

    def order_back(g):
        return (axis_x, axis_y) if g % 2 == BACK else (axis_y, axis_x)

    def index_of(seat):
        q = seat // per
        return (q if q < NEAR else CHUNKS - 1 + NEAR - q) * per + seat % per

    seat_of = index_of

    def step_z(i):
        return (z + NZ + ((i + 1) // 2) * (2 * (i % 2) - 1)) % NZ

    barrier = pltpu.get_barrier_semaphore()

    def greet(i, carry):
        zz = step_z(i)
        for cc in range(NC):
            pl.semaphore_signal(barrier, inc=1, device_id=(zz, cc, y, x), device_id_type=MESH)
        return carry

    for peer in (*x_to, *y_to, after, before, partner):
        pl.semaphore_signal(barrier, inc=1, device_id=peer, device_id_type=MESH)
    lax.fori_loop(1, NZ, greet, 0)

    loads = {}

    def load(name, src, dst):
        copy = pltpu.make_async_copy(src, dst, load_s.at[len(loads)])
        copy.start()
        loads[name] = copy

    own_cols = pl.ds(pl.multiple_of(tp * LANE, LANE), LANE)
    w_rows = pl.ds(pl.multiple_of((c * WZ + z % WZ) * wrow, wrow), wrow)
    load("tokens", ffn_in, tokens)
    load("ffn_gain", ffn_gain_h, ffn_gain)
    load("routes", routes_h, routes_t)
    load("weight", weight_h, weight_t)
    load("out_w", out_w.at[w_rows], full_w.at[w_rows, own_cols])
    load("branch", branch, ext.at[pl.ds(RIM, rows_a)])
    load("pool_w", pool_w_h, pool_w)
    load("group_gain", group_gain_h, group_gain)
    load("out_gain", out_gain_h, out_gain)

    for a in range(NY):
        for b in range(NX):
            here, there = (a * NX + b) * LANE, (b * NY + a) * LANE
            load(("down", 0, a, b), down_w.at[0, :, pl.ds(here, LANE)], down.at[1, :, pl.ds(there, LANE)])
            for k, w in enumerate((gate_w, up_w)):
                load(
                    ("gate_up", k, a, b),
                    w.at[0, pl.ds(here, LANE)],
                    gate_up.at[1, pl.ds(there, LANE), pl.ds(k * hid, hid)],
                )
    load(("down", 1), down_w.at[0], down.at[0])
    for k, w in enumerate((gate_w, up_w)):
        load(("gate_up", k), w.at[0], gate_up.at[0, :, pl.ds(k * hid, hid)])

    loads["tokens"].wait()
    acc = jnp.zeros((rows_b, LANE), F32)
    for k in range(model // LANE):
        v = tokens[:, k * LANE : (k + 1) * LANE].astype(F32)
        acc = acc + v * v
    scale = lax.rsqrt(jnp.sum(acc, axis=1, keepdims=True) * (1.0 / model) + norm_eps)
    loads["ffn_gain"].wait()
    normed = (tokens[:, own_cols].astype(F32) * scale * ffn_gain[:, own_cols]).astype(BF)

    loads["routes"].wait()
    loads["weight"].wait()
    experts = NZ * NC
    ids = lax.broadcasted_iota(jnp.int32, (experts, rows_b), 0)
    named = jnp.zeros((experts, rows_b), F32)
    weight = jnp.zeros((experts, rows_b), F32)
    for k in range(routes_t.shape[0]):
        hit = ids == routes_t[k : k + 1, :]
        named = named + jnp.where(hit, 1.0, 0.0)
        weight = weight + jnp.where(hit, weight_t[k : k + 1, :], 0.0)
    earlier = jnp.where(
        lax.broadcasted_iota(jnp.int32, (rows_b, rows_b), 0)
        < lax.broadcasted_iota(jnp.int32, (rows_b, rows_b), 1),
        1.0,
        0.0,
    ).astype(BF)
    place_of = jnp.where(named > 0.5, dot(named.astype(BF), earlier), -1.0)
    slot_ids = lax.broadcasted_iota(jnp.int32, (CAP, rows_b), 0).astype(F32)
    for e in range(experts):
        hot[e * CAP : (e + 1) * CAP, :] = jnp.where(slot_ids == place_of[e : e + 1, :], 1.0, 0.0).astype(BF)
    picked[...] = dot(hot[...], normed).astype(BF)
    loads["out_w"].wait()
    loads["branch"].wait()

    pl.semaphore_wait(barrier, 2 * (NZ - 1) + 7)

    sends = []

    def push(src, dst, sems, index, peer):
        send, recv = sems
        copy = pltpu.make_async_remote_copy(
            src,
            dst,
            send_sem=send.at[index],
            recv_sem=recv.at[index],
            device_id=peer,
            device_id_type=MESH,
        )
        copy.start()
        sends.append(copy)
        return copy

    def lanes(which, count):
        return pl.ds(pl.multiple_of(which * count, count), count)

    gather = {}

    def w_block(k, d=None, where=0):
        first, count = (c * WZ + (z + (k if where == 2 else 0) + NZ) % WZ) * wrow, wrow
        if d is not None:
            first, count = first + d * (wrow // 2), wrow // 2
        rows = pl.ds(pl.multiple_of(first, count), count)
        if where == 0:
            return full_w.at[rows, lanes(y * NX + (x + k + NX) % NX, LANE)]
        if where == 1:
            return full_w.at[rows, lanes((y + k + NY) % NY, wide)]
        return full_w.at[rows]

    w_axes = (x_to, y_to, z_to)

    def w_first(where):
        ref = w_block(0, None, where)
        gather["w", where, 0] = [
            push(ref, ref, (w_s, w_r), where * 4 + d, w_axes[where][d]) for d in range(2)
        ]

    def w_second(where):
        out = []
        for d in range(2):
            gather["w", where, 0][d].wait_recv()
            ref = w_block(2 * d - 1, d, where)
            out.append(push(ref, ref, (w_s, w_r), where * 4 + 2 + d, w_axes[where][d]))
        gather["w", where, 1] = out

    def w_third(where):
        for d in range(2):
            gather["w", where, 1][d].wait_recv()

    def w1():
        w_first(0)

    def w2():
        w_second(0)

    def w3():
        w_third(0)
        w_first(1)

    def w4():
        w_second(1)

    def w5():
        w_third(1)
        w_first(2)

    def w6():
        w_second(2)

    def w7():
        w_third(2)
        ref = full_w.at[lanes(c, width // NC)]
        gather["swap"] = push(ref, ref, (w_s, w_r), 12, partner)

    def ag1(g):
        arrived(g)
        (a, a_to), (b, b_to) = order(g)
        rows = pl.ds(g * crow, crow)
        ref = full.at[rows, lanes(b * NX + a, LANE)]
        gather[g, 0] = [push(ref, ref, (ag_s, ag_r), g * 8 + d, a_to[d]) for d in range(2)]

    def ag2(g, d):
        (a, a_to), (b, b_to) = order(g)
        gather[g, 0][d].wait_recv()
        rows = pl.ds(g * crow + d * half, half)
        ref = full.at[rows, lanes(b * NX + (a + NX - 1 + 2 * d) % NX, LANE)]
        gather[g, 1, d] = push(ref, ref, (ag_s, ag_r), g * 8 + 2 + d, a_to[d])

    def ag3(g):
        (a, a_to), (b, b_to) = order(g)
        for d in range(2):
            gather[g, 1, d].wait_recv()
        ref = full.at[pl.ds(g * crow, crow), lanes(b, wide)]
        gather[g, 2] = [push(ref, ref, (ag_s, ag_r), g * 8 + 4 + d, b_to[d]) for d in range(2)]

    def ag4(g, d):
        (a, a_to), (b, b_to) = order(g)
        gather[g, 2][d].wait_recv()
        rows = pl.ds(g * crow + d * half, half)
        ref = full.at[rows, lanes((b + NY - 1 + 2 * d) % NY, wide)]
        gather[g, 3, d] = push(ref, ref, (ag_s, ag_r), g * 8 + 6 + d, b_to[d])

    def seat_ref(seat, cc):
        cols = lanes(tp_p if (seat // per) % 2 else tp, LANE)
        return full.at[lanes(seat * NC + cc, CAP), cols]

    own_pick = pltpu.make_async_copy(picked.at[lanes(ep, CAP)], seat_ref(seat_of(0), c), own_s.at[0])

    def dispatch(zz, cc, seat):
        return pltpu.make_async_remote_copy(
            picked.at[lanes(zz * NC + cc, CAP)],
            seat_ref(seat, c),
            send_sem=z_s.at[0],
            recv_sem=z_r.at[seat // per],
            device_id=(zz, cc, y, x),
            device_id_type=MESH,
        )

    def dispatch_all():
        for seat in range(NZ):
            i = index_of(seat)
            if i == 0:
                own_pick.start()
                dispatch(z, 1 - c, seat).start()
                continue
            back = min(i + 2 * (i % 2) - 1, NZ - 1)
            for cc in range(NC):
                dispatch(step_z(i), cc, seat_of(back)).start()

    def arrived(g):
        own = g == seat_of(0) // per
        ref = full.at[pl.ds(g * crow, crow - CAP if own else crow), 0:LANE]
        pltpu.make_async_copy(ref, ref, z_r.at[g]).wait()
        if own:
            own_pick.wait()

    def pool_mix():
        gather["rim"].wait_recv()
        for name in ("pool_w", "group_gain", "out_gain"):
            loads[name].wait()
        reach = rows_a + RIM
        row = lax.broadcasted_iota(jnp.int32, (rows_a, reach), 0) + RIM
        col = lax.broadcasted_iota(jnp.int32, (rows_a, reach), 1)
        first = jnp.where(spot == 0, RIM, 0)
        age = jnp.where(col < first, reach, row - col)
        position = spot * rows_a + lax.broadcasted_iota(jnp.int32, (rows_a, LANE), 0)
        parts = []
        acc = jnp.zeros((rows_a, LANE), F32)
        for k, window in enumerate(pool_windows):
            cols = slice(k * LANE, (k + 1) * LANE)
            band = jnp.where((age >= 0) & (age < window), 1.0, 0.0).astype(BF)
            summed = dot(band, ext[:, cols])
            count = jnp.minimum(position + 1, window).astype(F32)
            pooled = (summed / count - ext[RIM:, cols].astype(F32)).astype(BF)
            mix = dot(pooled, pool_w[k])
            parts.append(mix)
            acc = acc + mix * mix
        scale = lax.rsqrt(jnp.sum(acc, axis=1, keepdims=True) * (1.0 / width) + norm_eps)
        for k, mix in enumerate(parts):
            cols = slice(k * LANE, (k + 1) * LANE)
            mixed[:, cols] = (mix * scale * group_gain[:, cols]).astype(BF)

    store = pltpu.make_async_copy(mixer, mixer_out, own_s.at[2])

    def pool_out():
        gather["swap"].wait_recv()
        acc = jnp.zeros((rows_a, LANE), F32)
        tile = 256
        for n in range(model // tile):
            cols = slice(n * tile, (n + 1) * tile)
            v = dot(mixed[...], full_w[:, cols])
            proj[:, cols] = v
            for k in range(tile // LANE):
                w = v[:, k * LANE : (k + 1) * LANE]
                acc = acc + w * w
        scale = lax.rsqrt(jnp.sum(acc, axis=1, keepdims=True) * (1.0 / model) + norm_eps)
        for n in range(model // tile):
            cols = slice(n * tile, (n + 1) * tile)
            mixer[:, cols] = (proj[:, cols] * scale * out_gain[:, cols]).astype(BF)
        store.start()

    def weigh():
        for e in range(0, experts, LANE // CAP):
            rows = []
            for k in range(LANE // CAP):
                h = hot[(e + k) * CAP : (e + k + 1) * CAP, :].astype(F32)
                rows.append(h * weight[e + k : e + k + 1, :])
            turned = jnp.concatenate(rows, axis=0).T
            high = turned.astype(BF)
            cols = slice(e * CAP, e * CAP + LANE)
            w_hi[:, cols] = high
            w_lo[:, cols] = (turned - high.astype(F32)).astype(BF)

    reduce = {}

    def block(which, count):
        return lanes(which % NX, count)

    def down_block(g, k):
        (a, a_to), (b, b_to) = order_back(g)
        rows, cols = pl.ds(g * crow, crow), block(a + 2 + k, wide)
        part[rows, cols] = dot(hidden[rows, :], down[1 if g % 2 == BACK else 0, :, cols]).astype(BF)
        return cols

    def c1(g):
        (a, a_to), (b, b_to) = order_back(g)
        for d in range(2):
            gather[g, 3, d].wait_recv()
        for name in tuple(loads):
            if isinstance(name, tuple):
                loads.pop(name).wait()
        r = g * crow
        both = dot(full[r : r + crow, :], gate_up[g % 2])
        gate = jnp.minimum(both[:, :hid], clamp_limit)
        up = jnp.clip(both[:, hid:], -clamp_limit, clamp_limit)
        hidden[r : r + crow, :] = ((up + 1.0) * gate * jax.nn.sigmoid(sigmoid_slope * gate)).astype(BF)
        cols = down_block(g, 0)
        reduce[g, 0] = [
            push(
                part.at[pl.ds(r + d * half, half), cols],
                rx1.at[pl.ds(r + d * half, half)],
                (rs_s, rs_r),
                g * 8 + d,
                a_to[d],
            )
            for d in range(2)
        ]

    def c2(g):
        for k in range(1, NX):
            down_block(g, k)

    def add(*values):
        out = values[0].astype(F32)
        for v in values[1:]:
            out = out + v.astype(F32)
        return out.astype(BF)

    def rs2(g, d):
        (a, a_to), (b, b_to) = order_back(g)
        r = g * crow
        reduce[g, 0][d].wait_recv()
        cols = block(a + 1 + 2 * d, wide)
        rows = slice(r + d * half, r + d * half + half)
        part[rows, cols] = add(part[rows, cols], rx1[rows, :])
        reduce[g, 1, d] = push(
            part.at[pl.ds(r, crow), cols],
            rx2.at[pl.ds(r, crow), pl.ds(d * wide, wide)],
            (rs_s, rs_r),
            g * 8 + 2 + d,
            a_to[d],
        )

    def rs3(g):
        (a, a_to), (b, b_to) = order_back(g)
        r = g * crow
        for d in range(2):
            reduce[g, 1, d].wait_recv()
        rows = slice(r, r + crow)
        sum_x[rows, :] = add(part[rows, block(a, wide)], rx2[rows, :wide], rx2[rows, wide:])
        cols = block(b + 2, LANE)
        reduce[g, 2] = [
            push(
                sum_x.at[pl.ds(r + d * half, half), cols],
                ry1.at[pl.ds(r + d * half, half)],
                (rs_s, rs_r),
                g * 8 + 4 + d,
                b_to[d],
            )
            for d in range(2)
        ]

    def rs4(g, d):
        (a, a_to), (b, b_to) = order_back(g)
        r = g * crow
        reduce[g, 2][d].wait_recv()
        cols = block(b + 1 + 2 * d, LANE)
        rows = slice(r + d * half, r + d * half + half)
        sum_x[rows, cols] = add(sum_x[rows, cols], ry1[rows, :])
        reduce[g, 3, d] = push(
            sum_x.at[pl.ds(r, crow), cols],
            ry2.at[pl.ds(r, crow), pl.ds(d * LANE, LANE)],
            (rs_s, rs_r),
            g * 8 + 6 + d,
            b_to[d],
        )

    own_rows = lanes(ep, CAP)
    own_back = pltpu.make_async_copy(
        home.at[lanes(seat_of(0) * NC + c, CAP)], result.at[own_rows], own_s.at[1]
    )

    def give_back(seat, cc):
        return pltpu.make_async_remote_copy(
            home.at[lanes(seat * NC + cc, CAP)],
            result.at[own_rows],
            send_sem=back_s.at[0],
            recv_sem=back_r.at[0],
            device_id=(step_z(index_of(seat)), cc, y, x),
            device_id_type=MESH,
        )

    def rs5(g):
        (a, a_to), (b, b_to) = order_back(g)
        r = g * crow
        for d in range(2):
            reduce[g, 3, d].wait_recv()
        rows = slice(r, r + crow)
        home[rows, :] = add(sum_x[rows, block(b, LANE)], ry2[rows, :LANE], ry2[rows, LANE:])
        for seat in range(g * per, (g + 1) * per):
            if index_of(seat) == 0:
                own_back.start()
                give_back(seat, 1 - c).start()
                continue
            for cc in range(NC):
                give_back(seat, cc).start()

    gather["rim"] = push(ext.at[pl.ds(rows_a, RIM)], ext.at[pl.ds(0, RIM)], (w_s, w_r), 13, after)
    dispatch_all()

    steps = dict(
        w1=w1, w2=w2, w3=w3, w4=w4, w5=w5, w6=w6, w7=w7, pm=pool_mix, po=pool_out,
        ag1=ag1, ag2=ag2, ag3=ag3, ag4=ag4, c1=c1, c2=c2, rs2=rs2, rs3=rs3, rs4=rs4, rs5=rs5, wh=weigh,
    )
    for name, *where in ORDER:
        steps[name](*where)

    store.wait()
    own_back.wait()
    ref = result.at[pl.ds(0, slots - CAP)]
    pltpu.make_async_copy(ref, ref, back_r.at[0]).wait()
    value = dot(w_hi[...], result[...]) + dot(w_lo[...], result[...])
    answer[...] = value.astype(BF)
    last = pltpu.make_async_copy(answer, expert_out, own_s.at[3])
    last.start()
    for copy in sends:
        copy.wait_send()
    ref = picked.at[pl.ds(0, slots - CAP)]
    pltpu.make_async_copy(ref, ref, z_s.at[0]).wait()
    ref = home.at[pl.ds(0, slots - CAP)]
    pltpu.make_async_copy(ref, ref, back_s.at[0]).wait()
    last.wait()


def per_device(
    branch_in,
    pool_weight,
    group_gain,
    out_weight,
    out_gain,
    ffn_input,
    ffn_gain,
    routes,
    route_weight,
    gate_weight,
    up_weight,
    down_weight,
):
    rows_a, width = branch_in.shape
    rows_b, model = ffn_input.shape
    hid = gate_weight.shape[2]
    top = routes.shape[1]
    slots = NZ * NC * CAP
    wide = NY * LANE
    any_ = pl.BlockSpec(memory_space=pl.ANY)
    dma = pltpu.SemaphoreType.DMA
    return pl.pallas_call(
        kernel,
        name="mixer_and_experts",
        out_shape=(
            jax.ShapeDtypeStruct((rows_a, model), BF),
            jax.ShapeDtypeStruct((rows_b, LANE), BF),
        ),
        in_specs=[any_] * 12,
        out_specs=(any_, any_),
        scratch_shapes=[
            pltpu.VMEM(pool_weight.shape, BF),
            pltpu.VMEM((1, width), F32),
            pltpu.VMEM((1, model), F32),
            pltpu.VMEM((1, model), F32),
            pltpu.VMEM((top, rows_b), jnp.int32),
            pltpu.VMEM((top, rows_b), F32),
            pltpu.VMEM((slots, model), BF),
            pltpu.VMEM((width, model), BF),
            pltpu.VMEM((2, model, 2 * hid), BF),
            pltpu.VMEM((2, hid, model), BF),
            pltpu.VMEM((rows_a + RIM, width), BF),
            pltpu.VMEM((rows_a, width), BF),
            pltpu.VMEM((rows_a, model), F32),
            pltpu.VMEM((rows_a, model), BF),
            pltpu.VMEM((rows_b, model), BF),
            pltpu.VMEM((slots, rows_b), BF),
            pltpu.VMEM((slots, LANE), BF),
            pltpu.VMEM((slots, model), BF),
            pltpu.VMEM((slots, wide), BF),
            pltpu.VMEM((slots, 2 * wide), BF),
            pltpu.VMEM((slots, wide), BF),
            pltpu.VMEM((slots, LANE), BF),
            pltpu.VMEM((slots, 2 * LANE), BF),
            pltpu.VMEM((slots, LANE), BF),
            pltpu.VMEM((slots, LANE), BF),
            pltpu.VMEM((rows_b, LANE), BF),
            pltpu.VMEM((slots, hid), BF),
            pltpu.VMEM((rows_b, slots), BF),
            pltpu.VMEM((rows_b, slots), BF),
            dma((CHUNKS * 8,)),
            dma((CHUNKS * 8,)),
            dma((CHUNKS * 8,)),
            dma((CHUNKS * 8,)),
            dma((14,)),
            dma((14,)),
            dma((1,)),
            dma((CHUNKS,)),
            dma((1,)),
            dma((1,)),
            dma((4,)),
            dma((2,)),
            dma((64,)),
        ],
        compiler_params=pltpu.CompilerParams(collective_id=0, has_side_effects=True),
    )(
        branch_in,
        pool_weight,
        group_gain[None],
        out_weight,
        out_gain[None],
        ffn_input,
        ffn_gain[None],
        routes.T,
        route_weight.T,
        gate_weight,
        up_weight,
        down_weight,
    )


def solution(mesh):
    split = Mesh(mesh.devices.reshape(NZ, NC, NY, NX), AXES)
    in_specs = (
        P(AXES, None),
        P(),
        P(),
        P(None, TP),
        P(),
        P(EP, None),
        P(),
        P(EP, None),
        P(EP, None),
        P(EP, None, TP),
        P(EP, None, TP),
        P(EP, TP, None),
    )
    out_specs = (P(AXES, None), P(EP, TP))
    return jax.shard_map(
        per_device, mesh=split, in_specs=in_specs, out_specs=out_specs, check_vma=False
    )
```

```python
import functools

import jax
import jax.numpy as jnp
from jax import lax
from jax.experimental import pallas as pl
from jax.experimental.pallas import tpu as pltpu
from jax.sharding import Mesh
from jax.sharding import PartitionSpec as P

MESH = pl.DeviceIdType.MESH
AXES = ("z", "c", "y", "x")
EP = ("z", "c")
TP = ("y", "x")

pool_windows = (2, 4, 8, 16)
norm_eps = 1e-06
clamp_limit = 7.0
sigmoid_slope = 1.702

BF = jnp.bfloat16
F32 = jnp.float32

NZ, NC, NY, NX = 16, 2, 4, 4
CAP = 32
LANE = 128
CHUNKS = 8
NEAR = 8
SHARED = {"down": 9, "gate_up": 10}
RIM = 16
WZ = 4
BACK = 1
ORDER = (
    ("ag1", 0), ("ag1", 1), ("ag2", 0, 0), ("ag2", 0, 1), ("ag1", 2), ("ag2", 1, 0), ("ag2", 1, 1), ("w2",),
    ("ag3", 0), ("ag1", 3), ("ag1", 4), ("ag2", 2, 0), ("ag2", 2, 1), ("ag3", 1), ("ag1", 5), ("ag4", 0, 0),
    ("ag4", 0, 1), ("ag1", 6), ("ag1", 7), ("ag2", 3, 0), ("ag2", 3, 1), ("ag3", 2), ("ag4", 1, 0),
    ("ag4", 1, 1), ("pm",), ("ag2", 5, 0), ("ag2", 5, 1), ("w3",), ("ag2", 6, 0), ("ag2", 6, 1),
    ("ag2", 4, 0), ("ag3", 3), ("ag2", 7, 0), ("ag2", 7, 1), ("ag2", 4, 1), ("ag3", 5), ("ag4", 2, 0),
    ("ag4", 2, 1), ("ag3", 6), ("ag4", 3, 1), ("ag4", 3, 0), ("ag3", 7), ("ag3", 4), ("c1", 1),
    ("ag4", 5, 0), ("c1", 0), ("ag4", 5, 1), ("c2", 0), ("w4",), ("c2", 1), ("ag4", 6, 0), ("ag4", 6, 1),
    ("ag4", 7, 0), ("ag4", 7, 1), ("ag4", 4, 0), ("ag4", 4, 1), ("c1", 3), ("c2", 3), ("rs2", 0, 0),
    ("rs2", 0, 1), ("c1", 5), ("c2", 5), ("c1", 7), ("c2", 7), ("c1", 6), ("rs2", 3, 0), ("rs2", 3, 1),
    ("c2", 6), ("w5",), ("c1", 4), ("c2", 4), ("rs3", 0), ("c1", 2), ("c2", 2), ("rs2", 7, 0),
    ("rs2", 7, 1), ("rs2", 6, 0), ("rs2", 6, 1), ("rs3", 3), ("rs4", 0, 0), ("rs4", 0, 1), ("rs2", 5, 0),
    ("rs2", 5, 1), ("rs2", 4, 0), ("rs2", 4, 1), ("rs3", 7), ("rs5", 0), ("rs3", 6), ("rs4", 3, 0),
    ("rs4", 3, 1), ("rs2", 1, 0), ("rs2", 1, 1), ("rs2", 2, 0), ("rs2", 2, 1), ("rs3", 5), ("w6",),
    ("rs4", 6, 0), ("rs4", 6, 1), ("rs3", 4), ("rs4", 7, 0), ("rs4", 7, 1), ("rs5", 3), ("rs3", 1),
    ("rs5", 6), ("rs4", 4, 0), ("rs4", 4, 1), ("rs3", 2), ("rs4", 5, 0), ("rs4", 5, 1), ("rs5", 7),
    ("rs4", 1, 0), ("rs4", 1, 1), ("rs5", 4), ("rs4", 2, 0), ("rs4", 2, 1), ("rs5", 5), ("rs5", 1), ("w7",),
    ("rs5", 2), ("po",), ("wh",),
)


def dot(a, b):
    return jnp.dot(a, b, preferred_element_type=F32)


def kernel(
    branch,
    pool_w_h,
    group_gain_h,
    out_w,
    out_gain_h,
    ffn_in,
    ffn_gain_h,
    routes_h,
    weight_h,
    gate_w,
    up_w,
    down_w,
    mixer_out,
    expert_out,
    pool_w,
    group_gain,
    out_gain,
    ffn_gain,
    routes_t,
    weight_t,
    full,
    full_w,
    gate_up,
    down,
    ext,
    mixed,
    proj,
    mixer,
    tokens,
    hot,
    picked,
    part,
    rx1,
    rx2,
    sum_x,
    ry1,
    ry2,
    home,
    result,
    answer,
    hidden,
    w_hi,
    w_lo,
    ag_s,
    ag_r,
    rs_s,
    rs_r,
    w_s,
    w_r,
    z_s,
    z_r,
    back_s,
    back_r,
    own_s,
    load_s,
):
    z, c = lax.axis_index("z"), lax.axis_index("c")
    y, x = lax.axis_index("y"), lax.axis_index("x")
    ep = z * NC + c
    tp = y * NX + x
    tp_p = x * NY + y
    rows_a = branch.shape[0]
    rows_b = ffn_in.shape[0]
    model = ffn_in.shape[1]
    hid = gate_w.shape[2]
    width = branch.shape[1]
    slots = NZ * NC * CAP
    crow = slots // CHUNKS
    half = crow // 2
    per = NZ // CHUNKS
    wide = NY * LANE
    wrow = width // (NC * WZ)

    spot = (ep * NY + y) * NX + x
    total = NZ * NC * NY * NX

    def place(index):
        return (index // (NC * NY * NX), (index // (NY * NX)) % NC, (index // NX) % NY, index % NX)

    after = place((spot + 1) % total)
    before = place((spot + total - 1) % total)
    x_to = ((z, c, y, (x + 1) % NX), (z, c, y, (x + NX - 1) % NX))
    y_to = ((z, c, (y + 1) % NY, x), (z, c, (y + NY - 1) % NY, x))
    z_to = (((z + 1) % NZ, c, y, x), ((z + NZ - 1) % NZ, c, y, x))
    partner = (z, 1 - c, y, x)
    axis_x = (x, x_to)
    axis_y = (y, y_to)

    def order(g):
        return (axis_x, axis_y) if g % 2 == 0 else (axis_y, axis_x)

    def order_back(g):
        return (axis_x, axis_y) if g % 2 == BACK else (axis_y, axis_x)

    def index_of(seat):
        q = seat // per
        return (q if q < NEAR else CHUNKS - 1 + NEAR - q) * per + seat % per

    seat_of = index_of

    def step_z(i):
        return (z + NZ + ((i + 1) // 2) * (2 * (i % 2) - 1)) % NZ

    barrier = pltpu.get_barrier_semaphore()

    def greet(i, carry):
        zz = step_z(i)
        for cc in range(NC):
            pl.semaphore_signal(barrier, inc=1, device_id=(zz, cc, y, x), device_id_type=MESH)
        return carry

    for peer in (*x_to, *y_to, after, before, partner):
        pl.semaphore_signal(barrier, inc=1, device_id=peer, device_id_type=MESH)
    lax.fori_loop(1, NZ, greet, 0)

    loads = {}

    def load(name, src, dst):
        copy = pltpu.make_async_copy(src, dst, load_s.at[SHARED.get(name, len(loads))])
        copy.start()
        if name not in SHARED:
            loads[name] = copy

    own_cols = pl.ds(pl.multiple_of(tp * LANE, LANE), LANE)
    w_rows = pl.ds(pl.multiple_of((c * WZ + z % WZ) * wrow, wrow), wrow)
    load("tokens", ffn_in, tokens)
    load("ffn_gain", ffn_gain_h, ffn_gain)
    load("routes", routes_h, routes_t)
    load("weight", weight_h, weight_t)
    load("out_w", out_w.at[w_rows], full_w.at[w_rows, own_cols])
    load("branch", branch, ext.at[pl.ds(RIM, rows_a)])
    load("pool_w", pool_w_h, pool_w)
    load("group_gain", group_gain_h, group_gain)
    load("out_gain", out_gain_h, out_gain)

    for a in range(NY):
        for b in range(NX):
            here, there = (a * NX + b) * LANE, (b * NY + a) * LANE
            load("down", down_w.at[0, :, pl.ds(here, LANE)], down.at[1, :, pl.ds(there, LANE)])
            for k, w in enumerate((gate_w, up_w)):
                load(
                    "gate_up",
                    w.at[0, pl.ds(here, LANE)],
                    gate_up.at[1, pl.ds(there, LANE), pl.ds(k * hid, hid)],
                )
    load("down", down_w.at[0], down.at[0])
    for k, w in enumerate((gate_w, up_w)):
        load("gate_up", w.at[0], gate_up.at[0, :, pl.ds(k * hid, hid)])

    loads["tokens"].wait()
    acc = jnp.zeros((rows_b, LANE), F32)
    for k in range(model // LANE):
        v = tokens[:, k * LANE : (k + 1) * LANE].astype(F32)
        acc = acc + v * v
    scale = lax.rsqrt(jnp.sum(acc, axis=1, keepdims=True) * (1.0 / model) + norm_eps)
    loads["ffn_gain"].wait()
    normed = (tokens[:, own_cols].astype(F32) * scale * ffn_gain[:, own_cols]).astype(BF)

    loads["routes"].wait()
    loads["weight"].wait()
    experts = NZ * NC
    ids = lax.broadcasted_iota(jnp.int32, (experts, rows_b), 0)
    named = jnp.zeros((experts, rows_b), F32)
    weight = jnp.zeros((experts, rows_b), F32)
    for k in range(routes_t.shape[0]):
        hit = ids == routes_t[k : k + 1, :]
        named = named + jnp.where(hit, 1.0, 0.0)
        weight = weight + jnp.where(hit, weight_t[k : k + 1, :], 0.0)
    earlier = jnp.where(
        lax.broadcasted_iota(jnp.int32, (rows_b, rows_b), 0)
        < lax.broadcasted_iota(jnp.int32, (rows_b, rows_b), 1),
        1.0,
        0.0,
    ).astype(BF)
    place_of = jnp.where(named > 0.5, dot(named.astype(BF), earlier), -1.0)
    slot_ids = lax.broadcasted_iota(jnp.int32, (CAP, rows_b), 0).astype(F32)
    for e in range(experts):
        hot[e * CAP : (e + 1) * CAP, :] = jnp.where(slot_ids == place_of[e : e + 1, :], 1.0, 0.0).astype(BF)
    picked[...] = dot(hot[...], normed).astype(BF)
    loads["out_w"].wait()
    loads["branch"].wait()

    pl.semaphore_wait(barrier, 2 * (NZ - 1) + 7)

    def push(src, dst, sems, index, peer):
        (send, recv), (out, into) = sems, index
        copy = pltpu.make_async_remote_copy(
            src,
            dst,
            send_sem=send.at[out],
            recv_sem=recv.at[into],
            device_id=peer,
            device_id_type=MESH,
        )
        copy.start()
        return copy

    def lanes(which, count):
        return pl.ds(pl.multiple_of(which * count, count), count)

    gather = {}

    def w_block(k, d=None, where=0):
        first, count = (c * WZ + (z + (k if where == 2 else 0) + NZ) % WZ) * wrow, wrow
        if d is not None:
            first, count = first + d * (wrow // 2), wrow // 2
        rows = pl.ds(pl.multiple_of(first, count), count)
        if where == 0:
            return full_w.at[rows, lanes(y * NX + (x + k + NX) % NX, LANE)]
        if where == 1:
            return full_w.at[rows, lanes((y + k + NY) % NY, wide)]
        return full_w.at[rows]

    w_axes = (x_to, y_to, z_to)

    def w_first(where):
        ref = w_block(0, None, where)
        gather["w", where, 0] = [
            push(ref, ref, (w_s, w_r), (where, where * 4 + d), w_axes[where][d]) for d in range(2)
        ]

    def w_second(where):
        out = []
        for d in range(2):
            gather["w", where, 0][d].wait_recv()
            ref = w_block(2 * d - 1, d, where)
            out.append(push(ref, ref, (w_s, w_r), (where, where * 4 + 2 + d), w_axes[where][d]))
        gather["w", where, 1] = out

    def w_third(where):
        for d in range(2):
            gather["w", where, 1][d].wait_recv()

    def w1():
        w_first(0)

    def w2():
        w_second(0)

    def w3():
        w_third(0)
        w_first(1)

    def w4():
        w_second(1)

    def w5():
        w_third(1)
        w_first(2)

    def w6():
        w_second(2)

    def w7():
        w_third(2)
        ref = full_w.at[lanes(c, width // NC)]
        gather["swap"] = push(ref, ref, (w_s, w_r), (3, 12), partner)

    def spread(g, which):
        (a, a_to), (b, b_to) = order(g)
        ref = full.at[pl.ds(g * crow, crow), lanes(b * NX + which % NX, LANE)]
        for d in range(2):
            push(ref, ref, (ag_s, ag_r), (0, g * 8 + 4 + d), b_to[d])

    def ag1(g):
        arrived(g)
        (a, a_to), (b, b_to) = order(g)
        rows = pl.ds(g * crow, crow)
        ref = full.at[rows, lanes(b * NX + a, LANE)]
        gather[g, 0] = [push(ref, ref, (ag_s, ag_r), (0, g * 8 + d), a_to[d]) for d in range(2)]
        spread(g, a)

    def ag2(g, d):
        (a, a_to), (b, b_to) = order(g)
        gather[g, 0][d].wait_recv()
        which = a + NX - 1 + 2 * d
        rows = pl.ds(g * crow + d * half, half)
        ref = full.at[rows, lanes(b * NX + which % NX, LANE)]
        gather[g, 1, d] = push(ref, ref, (ag_s, ag_r), (0, g * 8 + 2 + d), a_to[d])
        spread(g, which)

    def ag3(g):
        (a, a_to), (b, b_to) = order(g)
        for d in range(2):
            gather[g, 1, d].wait_recv()
        spread(g, a + 2)

    def ag4(g, d):
        (a, a_to), (b, b_to) = order(g)
        row = full.at[pl.ds(g * crow, crow), 0:wide]
        pltpu.make_async_copy(row, row, ag_r.at[g * 8 + 4 + d]).wait()
        rows = pl.ds(g * crow + d * half, half)
        ref = full.at[rows, lanes((b + NY - 1 + 2 * d) % NY, wide)]
        gather[g, 3, d] = push(ref, ref, (ag_s, ag_r), (0, g * 8 + 6 + d), b_to[d])

    def seat_ref(seat, cc):
        cols = lanes(tp_p if (seat // per) % 2 else tp, LANE)
        return full.at[lanes(seat * NC + cc, CAP), cols]

    own_pick = pltpu.make_async_copy(picked.at[lanes(ep, CAP)], seat_ref(seat_of(0), c), own_s.at[0])

    def dispatch(zz, cc, seat):
        return pltpu.make_async_remote_copy(
            picked.at[lanes(zz * NC + cc, CAP)],
            seat_ref(seat, c),
            send_sem=z_s.at[0],
            recv_sem=z_r.at[seat // per],
            device_id=(zz, cc, y, x),
            device_id_type=MESH,
        )

    def dispatch_all():
        for seat in range(NZ):
            i = index_of(seat)
            if i == 0:
                own_pick.start()
                dispatch(z, 1 - c, seat).start()
                continue
            back = min(i + 2 * (i % 2) - 1, NZ - 1)
            for cc in range(NC):
                dispatch(step_z(i), cc, seat_of(back)).start()

    def arrived(g):
        own = g == seat_of(0) // per
        ref = full.at[pl.ds(g * crow, crow - CAP if own else crow), 0:LANE]
        pltpu.make_async_copy(ref, ref, z_r.at[g]).wait()
        if own:
            own_pick.wait()

    def pool_mix():
        gather["rim"].wait_recv()
        for name in ("pool_w", "group_gain", "out_gain"):
            loads[name].wait()
        reach = rows_a + RIM
        row = lax.broadcasted_iota(jnp.int32, (rows_a, reach), 0) + RIM
        col = lax.broadcasted_iota(jnp.int32, (rows_a, reach), 1)
        first = jnp.where(spot == 0, RIM, 0)
        age = jnp.where(col < first, reach, row - col)
        position = spot * rows_a + lax.broadcasted_iota(jnp.int32, (rows_a, LANE), 0)
        parts = []
        acc = jnp.zeros((rows_a, LANE), F32)
        for k, window in enumerate(pool_windows):
            cols = slice(k * LANE, (k + 1) * LANE)
            band = jnp.where((age >= 0) & (age < window), 1.0, 0.0).astype(BF)
            summed = dot(band, ext[:, cols])
            count = jnp.minimum(position + 1, window).astype(F32)
            pooled = (summed / count - ext[RIM:, cols].astype(F32)).astype(BF)
            mix = dot(pooled, pool_w[k])
            parts.append(mix)
            acc = acc + mix * mix
        scale = lax.rsqrt(jnp.sum(acc, axis=1, keepdims=True) * (1.0 / width) + norm_eps)
        for k, mix in enumerate(parts):
            cols = slice(k * LANE, (k + 1) * LANE)
            mixed[:, cols] = (mix * scale * group_gain[:, cols]).astype(BF)

    store = pltpu.make_async_copy(mixer, mixer_out, own_s.at[2])

    def pool_out():
        gather["swap"].wait_recv()
        acc = jnp.zeros((rows_a, LANE), F32)
        tile = 256
        for n in range(model // tile):
            cols = slice(n * tile, (n + 1) * tile)
            v = dot(mixed[...], full_w[:, cols])
            proj[:, cols] = v
            for k in range(tile // LANE):
                w = v[:, k * LANE : (k + 1) * LANE]
                acc = acc + w * w
        scale = lax.rsqrt(jnp.sum(acc, axis=1, keepdims=True) * (1.0 / model) + norm_eps)
        for n in range(model // tile):
            cols = slice(n * tile, (n + 1) * tile)
            mixer[:, cols] = (proj[:, cols] * scale * out_gain[:, cols]).astype(BF)
        store.start()

    def weigh():
        for e in range(0, experts, LANE // CAP):
            rows = []
            for k in range(LANE // CAP):
                h = hot[(e + k) * CAP : (e + k + 1) * CAP, :].astype(F32)
                rows.append(h * weight[e + k : e + k + 1, :])
            turned = jnp.concatenate(rows, axis=0).T
            high = turned.astype(BF)
            cols = slice(e * CAP, e * CAP + LANE)
            w_hi[:, cols] = high
            w_lo[:, cols] = (turned - high.astype(F32)).astype(BF)

    reduce = {}

    def block(which, count):
        return lanes(which % NX, count)

    def down_block(g, k):
        (a, a_to), (b, b_to) = order_back(g)
        rows, cols = pl.ds(g * crow, crow), block(a + 2 + k, wide)
        part[rows, cols] = dot(hidden[rows, :], down[1 if g % 2 == BACK else 0, :, cols]).astype(BF)
        return cols

    def c1(g):
        (a, a_to), (b, b_to) = order_back(g)
        for d in range(2):
            gather[g, 3, d].wait_recv()
        if "weights" not in gather:
            gather["weights"] = True
            for ref, name in ((down, "down"), (gate_up, "gate_up")):
                pltpu.make_async_copy(ref, ref, load_s.at[SHARED[name]]).wait()
        r = g * crow
        both = dot(full[r : r + crow, :], gate_up[g % 2])
        gate = jnp.minimum(both[:, :hid], clamp_limit)
        up = jnp.clip(both[:, hid:], -clamp_limit, clamp_limit)
        hidden[r : r + crow, :] = ((up + 1.0) * gate * jax.nn.sigmoid(sigmoid_slope * gate)).astype(BF)
        cols = down_block(g, 0)
        reduce[g, 0] = [
            push(
                part.at[pl.ds(r + d * half, half), cols],
                rx1.at[pl.ds(r + d * half, half)],
                (rs_s, rs_r),
                (0, g * 8 + d),
                a_to[d],
            )
            for d in range(2)
        ]

    def c2(g):
        for k in range(1, NX):
            down_block(g, k)

    def add(*values):
        out = values[0].astype(F32)
        for v in values[1:]:
            out = out + v.astype(F32)
        return out.astype(BF)

    def rs2(g, d):
        (a, a_to), (b, b_to) = order_back(g)
        r = g * crow
        reduce[g, 0][d].wait_recv()
        cols = block(a + 1 + 2 * d, wide)
        rows = slice(r + d * half, r + d * half + half)
        part[rows, cols] = add(part[rows, cols], rx1[rows, :])
        reduce[g, 1, d] = push(
            part.at[pl.ds(r, crow), cols],
            rx2.at[pl.ds(r, crow), pl.ds(d * wide, wide)],
            (rs_s, rs_r),
            (0, g * 8 + 2 + d),
            a_to[d],
        )

    def rs3(g):
        (a, a_to), (b, b_to) = order_back(g)
        r = g * crow
        for d in range(2):
            reduce[g, 1, d].wait_recv()
        rows = slice(r, r + crow)
        sum_x[rows, :] = add(part[rows, block(a, wide)], rx2[rows, :wide], rx2[rows, wide:])
        cols = block(b + 2, LANE)
        reduce[g, 2] = [
            push(
                sum_x.at[pl.ds(r + d * half, half), cols],
                ry1.at[pl.ds(r + d * half, half)],
                (rs_s, rs_r),
                (0, g * 8 + 4 + d),
                b_to[d],
            )
            for d in range(2)
        ]

    def rs4(g, d):
        (a, a_to), (b, b_to) = order_back(g)
        r = g * crow
        reduce[g, 2][d].wait_recv()
        cols = block(b + 1 + 2 * d, LANE)
        rows = slice(r + d * half, r + d * half + half)
        sum_x[rows, cols] = add(sum_x[rows, cols], ry1[rows, :])
        reduce[g, 3, d] = push(
            sum_x.at[pl.ds(r, crow), cols],
            ry2.at[pl.ds(r, crow), pl.ds(d * LANE, LANE)],
            (rs_s, rs_r),
            (0, g * 8 + 6 + d),
            b_to[d],
        )

    own_rows = lanes(ep, CAP)
    own_back = pltpu.make_async_copy(
        home.at[lanes(seat_of(0) * NC + c, CAP)], result.at[own_rows], own_s.at[1]
    )

    def give_back(seat, cc):
        return pltpu.make_async_remote_copy(
            home.at[lanes(seat * NC + cc, CAP)],
            result.at[own_rows],
            send_sem=back_s.at[0],
            recv_sem=back_r.at[0],
            device_id=(step_z(index_of(seat)), cc, y, x),
            device_id_type=MESH,
        )

    def rs5(g):
        (a, a_to), (b, b_to) = order_back(g)
        r = g * crow
        for d in range(2):
            reduce[g, 3, d].wait_recv()
        rows = slice(r, r + crow)
        home[rows, :] = add(sum_x[rows, block(b, LANE)], ry2[rows, :LANE], ry2[rows, LANE:])
        for seat in range(g * per, (g + 1) * per):
            if index_of(seat) == 0:
                own_back.start()
                give_back(seat, 1 - c).start()
                continue
            for cc in range(NC):
                give_back(seat, cc).start()

    gather["rim"] = push(ext.at[pl.ds(rows_a, RIM)], ext.at[pl.ds(0, RIM)], (w_s, w_r), (4, 13), after)
    w1()
    dispatch_all()

    steps = dict(
        w2=w2, w3=w3, w4=w4, w5=w5, w6=w6, w7=w7, pm=pool_mix, po=pool_out,
        ag1=ag1, ag2=ag2, ag3=ag3, ag4=ag4, c1=c1, c2=c2, rs2=rs2, rs3=rs3, rs4=rs4, rs5=rs5, wh=weigh,
    )
    for name, *where in ORDER:
        steps[name](*where)

    store.wait()
    own_back.wait()
    ref = result.at[pl.ds(0, slots - CAP)]
    pltpu.make_async_copy(ref, ref, back_r.at[0]).wait()
    value = dot(w_hi[...], result[...]) + dot(w_lo[...], result[...])
    answer[...] = value.astype(BF)
    last = pltpu.make_async_copy(answer, expert_out, own_s.at[3])
    last.start()
    for ref, sem in (
        (full.at[:, 0 : 3 * LANE + 3 * wide], ag_s.at[0]),
        (part.at[:, 0 : 3 * LANE + 3 * wide], rs_s.at[0]),
        (full_w.at[pl.ds(0, 3 * wrow), 0:LANE], w_s.at[0]),
        (full_w.at[pl.ds(0, 3 * wrow), 0:wide], w_s.at[1]),
        (full_w.at[pl.ds(0, 3 * wrow)], w_s.at[2]),
        (full_w.at[pl.ds(0, width // NC)], w_s.at[3]),
        (ext.at[pl.ds(0, RIM)], w_s.at[4]),
    ):
        pltpu.make_async_copy(ref, ref, sem).wait()
    ref = picked.at[pl.ds(0, slots - CAP)]
    pltpu.make_async_copy(ref, ref, z_s.at[0]).wait()
    ref = home.at[pl.ds(0, slots - CAP)]
    pltpu.make_async_copy(ref, ref, back_s.at[0]).wait()
    last.wait()


def per_device(
    branch_in,
    pool_weight,
    group_gain,
    out_weight,
    out_gain,
    ffn_input,
    ffn_gain,
    routes,
    route_weight,
    gate_weight,
    up_weight,
    down_weight,
):
    rows_a, width = branch_in.shape
    rows_b, model = ffn_input.shape
    hid = gate_weight.shape[2]
    top = routes.shape[1]
    slots = NZ * NC * CAP
    wide = NY * LANE
    any_ = pl.BlockSpec(memory_space=pl.ANY)
    dma = pltpu.SemaphoreType.DMA
    return pl.pallas_call(
        kernel,
        name="mixer_and_experts",
        out_shape=(
            jax.ShapeDtypeStruct((rows_a, model), BF),
            jax.ShapeDtypeStruct((rows_b, LANE), BF),
        ),
        in_specs=[any_] * 12,
        out_specs=(any_, any_),
        scratch_shapes=[
            pltpu.VMEM(pool_weight.shape, BF),
            pltpu.VMEM((1, width), F32),
            pltpu.VMEM((1, model), F32),
            pltpu.VMEM((1, model), F32),
            pltpu.VMEM((top, rows_b), jnp.int32),
            pltpu.VMEM((top, rows_b), F32),
            pltpu.VMEM((slots, model), BF),
            pltpu.VMEM((width, model), BF),
            pltpu.VMEM((2, model, 2 * hid), BF),
            pltpu.VMEM((2, hid, model), BF),
            pltpu.VMEM((rows_a + RIM, width), BF),
            pltpu.VMEM((rows_a, width), BF),
            pltpu.VMEM((rows_a, model), F32),
            pltpu.VMEM((rows_a, model), BF),
            pltpu.VMEM((rows_b, model), BF),
            pltpu.VMEM((slots, rows_b), BF),
            pltpu.VMEM((slots, LANE), BF),
            pltpu.VMEM((slots, model), BF),
            pltpu.VMEM((slots, wide), BF),
            pltpu.VMEM((slots, 2 * wide), BF),
            pltpu.VMEM((slots, wide), BF),
            pltpu.VMEM((slots, LANE), BF),
            pltpu.VMEM((slots, 2 * LANE), BF),
            pltpu.VMEM((slots, LANE), BF),
            pltpu.VMEM((slots, LANE), BF),
            pltpu.VMEM((rows_b, LANE), BF),
            pltpu.VMEM((slots, hid), BF),
            pltpu.VMEM((rows_b, slots), BF),
            pltpu.VMEM((rows_b, slots), BF),
            dma((1,)),
            dma((CHUNKS * 8,)),
            dma((1,)),
            dma((CHUNKS * 8,)),
            dma((5,)),
            dma((14,)),
            dma((1,)),
            dma((CHUNKS,)),
            dma((1,)),
            dma((1,)),
            dma((4,)),
            dma((11,)),
        ],
        compiler_params=pltpu.CompilerParams(collective_id=0, has_side_effects=True),
    )(
        branch_in,
        pool_weight,
        group_gain[None],
        out_weight,
        out_gain[None],
        ffn_input,
        ffn_gain[None],
        routes.T,
        route_weight.T,
        gate_weight,
        up_weight,
        down_weight,
    )


def solution(mesh):
    split = Mesh(mesh.devices.reshape(NZ, NC, NY, NX), AXES)
    in_specs = (
        P(AXES, None),
        P(),
        P(),
        P(None, TP),
        P(),
        P(EP, None),
        P(),
        P(EP, None),
        P(EP, None),
        P(EP, None, TP),
        P(EP, None, TP),
        P(EP, TP, None),
    )
    out_specs = (P(AXES, None), P(EP, TP))
    return jax.shard_map(
        per_device, mesh=split, in_specs=in_specs, out_specs=out_specs, check_vma=False
    )
```

```python
import functools

import jax
import jax.numpy as jnp
from jax import lax
from jax.experimental import pallas as pl
from jax.experimental.pallas import tpu as pltpu
from jax.sharding import Mesh
from jax.sharding import PartitionSpec as P

MESH = pl.DeviceIdType.MESH
AXES = ("z", "c", "y", "x")
EP = ("z", "c")
TP = ("y", "x")

pool_windows = (2, 4, 8, 16)
norm_eps = 1e-06
clamp_limit = 7.0
sigmoid_slope = 1.702

BF = jnp.bfloat16
F32 = jnp.float32

NZ, NC, NY, NX = 16, 2, 4, 4
CAP = 32
LANE = 128
CHUNKS = 8
NEAR = 8
SHARED = {"down": 9, "gate_up": 10}
RIM = 16
WZ = 4
BACK = 1
ORDER = (
    ("ag1", 0), ("ag1", 1), ("ag2", 0, 0), ("ag2", 0, 1), ("ag1", 2), ("ag2", 1, 0), ("ag2", 1, 1), ("w2",),
    ("ag3", 0), ("ag1", 3), ("ag1", 4), ("ag2", 2, 0), ("ag2", 2, 1), ("ag3", 1), ("ag1", 5), ("ag4", 0, 0),
    ("ag4", 0, 1), ("ag1", 6), ("ag1", 7), ("ag2", 3, 0), ("ag2", 3, 1), ("ag3", 2), ("ag4", 1, 0),
    ("ag4", 1, 1), ("pm",), ("ag2", 5, 0), ("ag2", 5, 1), ("w3",), ("ag2", 6, 0), ("ag2", 6, 1),
    ("ag2", 4, 0), ("ag3", 3), ("ag2", 7, 0), ("ag2", 7, 1), ("ag2", 4, 1), ("ag3", 5), ("ag4", 2, 0),
    ("ag4", 2, 1), ("ag3", 6), ("ag4", 3, 1), ("ag4", 3, 0), ("ag3", 7), ("ag3", 4), ("c1", 1),
    ("ag4", 5, 0), ("c1", 0), ("ag4", 5, 1), ("c2", 0), ("w4",), ("c2", 1), ("ag4", 6, 0), ("ag4", 6, 1),
    ("ag4", 7, 0), ("ag4", 7, 1), ("ag4", 4, 0), ("ag4", 4, 1), ("c1", 3), ("c2", 3), ("rs2", 0, 0),
    ("rs2", 0, 1), ("c1", 5), ("c2", 5), ("c1", 7), ("c2", 7), ("c1", 6), ("rs2", 3, 0), ("rs2", 3, 1),
    ("c2", 6), ("w5",), ("c1", 4), ("c2", 4), ("rs3", 0), ("c1", 2), ("c2", 2), ("rs2", 7, 0),
    ("rs2", 7, 1), ("rs2", 6, 0), ("rs2", 6, 1), ("rs3", 3), ("rs4", 0, 0), ("rs4", 0, 1), ("rs2", 5, 0),
    ("rs2", 5, 1), ("rs2", 4, 0), ("rs2", 4, 1), ("rs3", 7), ("rs5", 0), ("rs3", 6), ("rs4", 3, 0),
    ("rs4", 3, 1), ("rs2", 1, 0), ("rs2", 1, 1), ("rs2", 2, 0), ("rs2", 2, 1), ("rs3", 5), ("w6",),
    ("rs4", 6, 0), ("rs4", 6, 1), ("rs3", 4), ("rs4", 7, 0), ("rs4", 7, 1), ("rs5", 3), ("rs3", 1),
    ("rs5", 6), ("rs4", 4, 0), ("rs4", 4, 1), ("rs3", 2), ("rs4", 5, 0), ("rs4", 5, 1), ("rs5", 7),
    ("rs4", 1, 0), ("rs4", 1, 1), ("rs5", 4), ("rs4", 2, 0), ("rs4", 2, 1), ("rs5", 5), ("rs5", 1), ("w7",),
    ("rs5", 2), ("po",), ("wh",),
)


def dot(a, b):
    return jnp.dot(a, b, preferred_element_type=F32)


def kernel(
    branch,
    pool_w_h,
    group_gain_h,
    out_w,
    out_gain_h,
    ffn_in,
    ffn_gain_h,
    routes_h,
    weight_h,
    gate_w,
    up_w,
    down_w,
    mixer_out,
    expert_out,
    pool_w,
    group_gain,
    out_gain,
    ffn_gain,
    routes_t,
    weight_t,
    full,
    full_w,
    gate_up,
    down,
    ext,
    mixed,
    proj,
    tokens,
    hot,
    picked,
    part,
    rx1,
    rx2,
    sum_x,
    ry1,
    ry2,
    home,
    result,
    hidden,
    w_hi,
    w_lo,
    ag_s,
    ag_r,
    rs_s,
    rs_r,
    w_s,
    w_r,
    z_s,
    z_r,
    back_s,
    back_r,
    own_s,
    load_s,
):
    z, c = lax.axis_index("z"), lax.axis_index("c")
    y, x = lax.axis_index("y"), lax.axis_index("x")
    ep = z * NC + c
    tp = y * NX + x
    tp_p = x * NY + y
    rows_a = branch.shape[0]
    rows_b = ffn_in.shape[0]
    model = ffn_in.shape[1]
    hid = gate_w.shape[2]
    width = branch.shape[1]
    slots = NZ * NC * CAP
    crow = slots // CHUNKS
    half = crow // 2
    per = NZ // CHUNKS
    wide = NY * LANE
    wrow = width // (NC * WZ)

    spot = (ep * NY + y) * NX + x
    total = NZ * NC * NY * NX

    def place(index):
        return (index // (NC * NY * NX), (index // (NY * NX)) % NC, (index // NX) % NY, index % NX)

    after = place((spot + 1) % total)
    before = place((spot + total - 1) % total)
    x_to = ((z, c, y, (x + 1) % NX), (z, c, y, (x + NX - 1) % NX))
    y_to = ((z, c, (y + 1) % NY, x), (z, c, (y + NY - 1) % NY, x))
    z_to = (((z + 1) % NZ, c, y, x), ((z + NZ - 1) % NZ, c, y, x))
    partner = (z, 1 - c, y, x)
    axis_x = (x, x_to)
    axis_y = (y, y_to)

    def order(g):
        return (axis_x, axis_y) if g % 2 == 0 else (axis_y, axis_x)

    def order_back(g):
        return (axis_x, axis_y) if g % 2 == BACK else (axis_y, axis_x)

    def index_of(seat):
        q = seat // per
        return (q if q < NEAR else CHUNKS - 1 + NEAR - q) * per + seat % per

    seat_of = index_of

    def step_z(i):
        return (z + NZ + ((i + 1) // 2) * (2 * (i % 2) - 1)) % NZ

    barrier = pltpu.get_barrier_semaphore()

    def greet(i, carry):
        zz = step_z(i)
        for cc in range(NC):
            pl.semaphore_signal(barrier, inc=1, device_id=(zz, cc, y, x), device_id_type=MESH)
        return carry

    for peer in (*x_to, *y_to, after, before, partner):
        pl.semaphore_signal(barrier, inc=1, device_id=peer, device_id_type=MESH)
    lax.fori_loop(1, NZ, greet, 0)

    loads = {}

    def load(name, src, dst):
        copy = pltpu.make_async_copy(src, dst, load_s.at[SHARED.get(name, len(loads))])
        copy.start()
        if name not in SHARED:
            loads[name] = copy

    own_cols = pl.ds(pl.multiple_of(tp * LANE, LANE), LANE)
    w_rows = pl.ds(pl.multiple_of((c * WZ + z % WZ) * wrow, wrow), wrow)
    load("tokens", ffn_in, tokens)
    load("ffn_gain", ffn_gain_h, ffn_gain)
    load("routes", routes_h, routes_t)
    load("weight", weight_h, weight_t)
    load("out_w", out_w.at[w_rows], full_w.at[w_rows, own_cols])
    load("branch", branch, ext.at[pl.ds(RIM, rows_a)])
    load("pool_w", pool_w_h, pool_w)
    load("group_gain", group_gain_h, group_gain)
    load("out_gain", out_gain_h, out_gain)

    for a in range(NY):
        for b in range(NX):
            here, there = (a * NX + b) * LANE, (b * NY + a) * LANE
            load("down", down_w.at[0, :, pl.ds(here, LANE)], down.at[1, :, pl.ds(there, LANE)])
            for k, w in enumerate((gate_w, up_w)):
                load(
                    "gate_up",
                    w.at[0, pl.ds(here, LANE)],
                    gate_up.at[1, pl.ds(there, LANE), pl.ds(k * hid, hid)],
                )
    load("down", down_w.at[0], down.at[0])
    for k, w in enumerate((gate_w, up_w)):
        load("gate_up", w.at[0], gate_up.at[0, :, pl.ds(k * hid, hid)])

    loads["tokens"].wait()
    acc = jnp.zeros((rows_b, LANE), F32)
    for k in range(model // LANE):
        v = tokens[:, k * LANE : (k + 1) * LANE].astype(F32)
        acc = acc + v * v
    scale = lax.rsqrt(jnp.sum(acc, axis=1, keepdims=True) * (1.0 / model) + norm_eps)
    loads["ffn_gain"].wait()
    normed = (tokens[:, own_cols].astype(F32) * scale * ffn_gain[:, own_cols]).astype(BF)

    loads["routes"].wait()
    loads["weight"].wait()
    experts = NZ * NC
    ids = lax.broadcasted_iota(jnp.int32, (experts, rows_b), 0)
    named = jnp.zeros((experts, rows_b), F32)
    weight = jnp.zeros((experts, rows_b), F32)
    for k in range(routes_t.shape[0]):
        hit = ids == routes_t[k : k + 1, :]
        named = named + jnp.where(hit, 1.0, 0.0)
        weight = weight + jnp.where(hit, weight_t[k : k + 1, :], 0.0)
    earlier = jnp.where(
        lax.broadcasted_iota(jnp.int32, (rows_b, rows_b), 0)
        < lax.broadcasted_iota(jnp.int32, (rows_b, rows_b), 1),
        1.0,
        0.0,
    ).astype(BF)
    place_of = jnp.where(named > 0.5, dot(named.astype(BF), earlier), -1.0)
    slot_ids = lax.broadcasted_iota(jnp.int32, (CAP, rows_b), 0).astype(F32)
    for e in range(experts):
        hot[e * CAP : (e + 1) * CAP, :] = jnp.where(slot_ids == place_of[e : e + 1, :], 1.0, 0.0).astype(BF)
    picked[...] = dot(hot[...], normed).astype(BF)
    loads["out_w"].wait()
    loads["branch"].wait()

    pl.semaphore_wait(barrier, 2 * (NZ - 1) + 7)

    def push(src, dst, sems, index, peer):
        (send, recv), (out, into) = sems, index
        copy = pltpu.make_async_remote_copy(
            src,
            dst,
            send_sem=send.at[out],
            recv_sem=recv.at[into],
            device_id=peer,
            device_id_type=MESH,
        )
        copy.start()
        return copy

    def lanes(which, count):
        return pl.ds(pl.multiple_of(which * count, count), count)

    gather = {}

    def w_block(k, d=None, where=0):
        first, count = (c * WZ + (z + (k if where == 2 else 0) + NZ) % WZ) * wrow, wrow
        if d is not None:
            first, count = first + d * (wrow // 2), wrow // 2
        rows = pl.ds(pl.multiple_of(first, count), count)
        if where == 0:
            return full_w.at[rows, lanes(y * NX + (x + k + NX) % NX, LANE)]
        if where == 1:
            return full_w.at[rows, lanes((y + k + NY) % NY, wide)]
        return full_w.at[rows]

    w_axes = (x_to, y_to, z_to)

    def w_first(where):
        ref = w_block(0, None, where)
        gather["w", where, 0] = [
            push(ref, ref, (w_s, w_r), (where, where * 4 + d), w_axes[where][d]) for d in range(2)
        ]

    def w_second(where):
        out = []
        for d in range(2):
            gather["w", where, 0][d].wait_recv()
            ref = w_block(2 * d - 1, d, where)
            out.append(push(ref, ref, (w_s, w_r), (where, where * 4 + 2 + d), w_axes[where][d]))
        gather["w", where, 1] = out

    def w_third(where):
        for d in range(2):
            gather["w", where, 1][d].wait_recv()

    def w1():
        w_first(0)

    def w2():
        w_second(0)

    def w3():
        w_third(0)
        w_first(1)

    def w4():
        w_second(1)

    def w5():
        w_third(1)
        w_first(2)

    def w6():
        w_second(2)

    def w7():
        w_third(2)
        ref = full_w.at[lanes(c, width // NC)]
        gather["swap"] = push(ref, ref, (w_s, w_r), (3, 12), partner)

    def spread(g, which):
        (a, a_to), (b, b_to) = order(g)
        ref = full.at[pl.ds(g * crow, crow), lanes(b * NX + which % NX, LANE)]
        for d in range(2):
            push(ref, ref, (ag_s, ag_r), (0, g * 8 + 4 + d), b_to[d])

    def ag1(g):
        arrived(g)
        (a, a_to), (b, b_to) = order(g)
        rows = pl.ds(g * crow, crow)
        ref = full.at[rows, lanes(b * NX + a, LANE)]
        gather[g, 0] = [push(ref, ref, (ag_s, ag_r), (0, g * 8 + d), a_to[d]) for d in range(2)]
        spread(g, a)

    def ag2(g, d):
        (a, a_to), (b, b_to) = order(g)
        gather[g, 0][d].wait_recv()
        which = a + NX - 1 + 2 * d
        rows = pl.ds(g * crow + d * half, half)
        ref = full.at[rows, lanes(b * NX + which % NX, LANE)]
        gather[g, 1, d] = push(ref, ref, (ag_s, ag_r), (0, g * 8 + 2 + d), a_to[d])
        spread(g, which)

    def ag3(g):
        (a, a_to), (b, b_to) = order(g)
        for d in range(2):
            gather[g, 1, d].wait_recv()
        spread(g, a + 2)

    def ag4(g, d):
        (a, a_to), (b, b_to) = order(g)
        row = full.at[pl.ds(g * crow, crow), 0:wide]
        pltpu.make_async_copy(row, row, ag_r.at[g * 8 + 4 + d]).wait()
        rows = pl.ds(g * crow + d * half, half)
        ref = full.at[rows, lanes((b + NY - 1 + 2 * d) % NY, wide)]
        gather[g, 3, d] = push(ref, ref, (ag_s, ag_r), (0, g * 8 + 6 + d), b_to[d])

    def seat_ref(seat, cc):
        cols = lanes(tp_p if (seat // per) % 2 else tp, LANE)
        return full.at[lanes(seat * NC + cc, CAP), cols]

    own_pick = pltpu.make_async_copy(picked.at[lanes(ep, CAP)], seat_ref(seat_of(0), c), own_s.at[0])

    def dispatch(zz, cc, seat):
        return pltpu.make_async_remote_copy(
            picked.at[lanes(zz * NC + cc, CAP)],
            seat_ref(seat, c),
            send_sem=z_s.at[0],
            recv_sem=z_r.at[seat // per],
            device_id=(zz, cc, y, x),
            device_id_type=MESH,
        )

    def dispatch_all():
        for seat in range(NZ):
            i = index_of(seat)
            if i == 0:
                own_pick.start()
                dispatch(z, 1 - c, seat).start()
                continue
            back = min(i + 2 * (i % 2) - 1, NZ - 1)
            for cc in range(NC):
                dispatch(step_z(i), cc, seat_of(back)).start()

    def arrived(g):
        own = g == seat_of(0) // per
        ref = full.at[pl.ds(g * crow, crow - CAP if own else crow), 0:LANE]
        pltpu.make_async_copy(ref, ref, z_r.at[g]).wait()
        if own:
            own_pick.wait()

    def pool_mix():
        gather["rim"].wait_recv()
        for name in ("pool_w", "group_gain", "out_gain"):
            loads[name].wait()
        reach = rows_a + RIM
        row = lax.broadcasted_iota(jnp.int32, (rows_a, reach), 0) + RIM
        col = lax.broadcasted_iota(jnp.int32, (rows_a, reach), 1)
        first = jnp.where(spot == 0, RIM, 0)
        age = jnp.where(col < first, reach, row - col)
        position = spot * rows_a + lax.broadcasted_iota(jnp.int32, (rows_a, LANE), 0)
        parts = []
        acc = jnp.zeros((rows_a, LANE), F32)
        for k, window in enumerate(pool_windows):
            cols = slice(k * LANE, (k + 1) * LANE)
            band = jnp.where((age >= 0) & (age < window), 1.0, 0.0).astype(BF)
            summed = dot(band, ext[:, cols])
            count = jnp.minimum(position + 1, window).astype(F32)
            pooled = (summed / count - ext[RIM:, cols].astype(F32)).astype(BF)
            mix = dot(pooled, pool_w[k])
            parts.append(mix)
            acc = acc + mix * mix
        scale = lax.rsqrt(jnp.sum(acc, axis=1, keepdims=True) * (1.0 / width) + norm_eps)
        for k, mix in enumerate(parts):
            cols = slice(k * LANE, (k + 1) * LANE)
            mixed[:, cols] = (mix * scale * group_gain[:, cols]).astype(BF)

    def pool_out():
        gather["swap"].wait_recv()
        acc = jnp.zeros((rows_a, LANE), F32)
        tile = 256
        for n in range(model // tile):
            cols = slice(n * tile, (n + 1) * tile)
            v = dot(mixed[...], full_w[:, cols])
            proj[:, cols] = v
            for k in range(tile // LANE):
                w = v[:, k * LANE : (k + 1) * LANE]
                acc = acc + w * w
        scale = lax.rsqrt(jnp.sum(acc, axis=1, keepdims=True) * (1.0 / model) + norm_eps)
        for n in range(model // tile):
            cols = slice(n * tile, (n + 1) * tile)
            mixer_out[:, cols] = (proj[:, cols] * scale * out_gain[:, cols]).astype(BF)

    def weigh():
        for e in range(0, experts, LANE // CAP):
            rows = []
            for k in range(LANE // CAP):
                h = hot[(e + k) * CAP : (e + k + 1) * CAP, :].astype(F32)
                rows.append(h * weight[e + k : e + k + 1, :])
            turned = jnp.concatenate(rows, axis=0).T
            high = turned.astype(BF)
            cols = slice(e * CAP, e * CAP + LANE)
            w_hi[:, cols] = high
            w_lo[:, cols] = (turned - high.astype(F32)).astype(BF)

    reduce = {}

    def block(which, count):
        return lanes(which % NX, count)

    def down_block(g, k):
        (a, a_to), (b, b_to) = order_back(g)
        rows, cols = pl.ds(g * crow, crow), block(a + 2 + k, wide)
        part[rows, cols] = dot(hidden[rows, :], down[1 if g % 2 == BACK else 0, :, cols]).astype(BF)
        return cols

    def c1(g):
        (a, a_to), (b, b_to) = order_back(g)
        for d in range(2):
            gather[g, 3, d].wait_recv()
        if "weights" not in gather:
            gather["weights"] = True
            for ref, name in ((down, "down"), (gate_up, "gate_up")):
                pltpu.make_async_copy(ref, ref, load_s.at[SHARED[name]]).wait()
        r = g * crow
        both = dot(full[r : r + crow, :], gate_up[g % 2])
        gate = jnp.minimum(both[:, :hid], clamp_limit)
        up = jnp.clip(both[:, hid:], -clamp_limit, clamp_limit)
        hidden[r : r + crow, :] = ((up + 1.0) * gate * jax.nn.sigmoid(sigmoid_slope * gate)).astype(BF)
        cols = down_block(g, 0)
        reduce[g, 0] = [
            push(
                part.at[pl.ds(r + d * half, half), cols],
                rx1.at[pl.ds(r + d * half, half)],
                (rs_s, rs_r),
                (0, g * 8 + d),
                a_to[d],
            )
            for d in range(2)
        ]

    def c2(g):
        for k in range(1, NX):
            down_block(g, k)

    def add(*values):
        out = values[0].astype(F32)
        for v in values[1:]:
            out = out + v.astype(F32)
        return out.astype(BF)

    def rs2(g, d):
        (a, a_to), (b, b_to) = order_back(g)
        r = g * crow
        reduce[g, 0][d].wait_recv()
        cols = block(a + 1 + 2 * d, wide)
        rows = slice(r + d * half, r + d * half + half)
        part[rows, cols] = add(part[rows, cols], rx1[rows, :])
        reduce[g, 1, d] = push(
            part.at[pl.ds(r, crow), cols],
            rx2.at[pl.ds(r, crow), pl.ds(d * wide, wide)],
            (rs_s, rs_r),
            (0, g * 8 + 2 + d),
            a_to[d],
        )

    def rs3(g):
        (a, a_to), (b, b_to) = order_back(g)
        r = g * crow
        for d in range(2):
            reduce[g, 1, d].wait_recv()
        rows = slice(r, r + crow)
        sum_x[rows, :] = add(part[rows, block(a, wide)], rx2[rows, :wide], rx2[rows, wide:])
        cols = block(b + 2, LANE)
        reduce[g, 2] = [
            push(
                sum_x.at[pl.ds(r + d * half, half), cols],
                ry1.at[pl.ds(r + d * half, half)],
                (rs_s, rs_r),
                (0, g * 8 + 4 + d),
                b_to[d],
            )
            for d in range(2)
        ]

    def rs4(g, d):
        (a, a_to), (b, b_to) = order_back(g)
        r = g * crow
        reduce[g, 2][d].wait_recv()
        cols = block(b + 1 + 2 * d, LANE)
        rows = slice(r + d * half, r + d * half + half)
        sum_x[rows, cols] = add(sum_x[rows, cols], ry1[rows, :])
        reduce[g, 3, d] = push(
            sum_x.at[pl.ds(r, crow), cols],
            ry2.at[pl.ds(r, crow), pl.ds(d * LANE, LANE)],
            (rs_s, rs_r),
            (0, g * 8 + 6 + d),
            b_to[d],
        )

    own_rows = lanes(ep, CAP)
    own_back = pltpu.make_async_copy(
        home.at[lanes(seat_of(0) * NC + c, CAP)], result.at[own_rows], own_s.at[1]
    )

    def give_back(seat, cc):
        return pltpu.make_async_remote_copy(
            home.at[lanes(seat * NC + cc, CAP)],
            result.at[own_rows],
            send_sem=back_s.at[0],
            recv_sem=back_r.at[0],
            device_id=(step_z(index_of(seat)), cc, y, x),
            device_id_type=MESH,
        )

    def rs5(g):
        (a, a_to), (b, b_to) = order_back(g)
        r = g * crow
        for d in range(2):
            reduce[g, 3, d].wait_recv()
        rows = slice(r, r + crow)
        home[rows, :] = add(sum_x[rows, block(b, LANE)], ry2[rows, :LANE], ry2[rows, LANE:])
        for seat in range(g * per, (g + 1) * per):
            if index_of(seat) == 0:
                own_back.start()
                give_back(seat, 1 - c).start()
                continue
            for cc in range(NC):
                give_back(seat, cc).start()

    gather["rim"] = push(ext.at[pl.ds(rows_a, RIM)], ext.at[pl.ds(0, RIM)], (w_s, w_r), (4, 13), after)
    w1()
    dispatch_all()

    steps = dict(
        w2=w2, w3=w3, w4=w4, w5=w5, w6=w6, w7=w7, pm=pool_mix, po=pool_out,
        ag1=ag1, ag2=ag2, ag3=ag3, ag4=ag4, c1=c1, c2=c2, rs2=rs2, rs3=rs3, rs4=rs4, rs5=rs5, wh=weigh,
    )
    for name, *where in ORDER:
        steps[name](*where)

    own_back.wait()
    ref = result.at[pl.ds(0, slots - CAP)]
    pltpu.make_async_copy(ref, ref, back_r.at[0]).wait()
    value = dot(w_hi[...], result[...]) + dot(w_lo[...], result[...])
    expert_out[...] = value.astype(BF)
    for ref, sem in (
        (full.at[:, 0 : 3 * LANE + 3 * wide], ag_s.at[0]),
        (part.at[:, 0 : 3 * LANE + 3 * wide], rs_s.at[0]),
        (full_w.at[pl.ds(0, 3 * wrow), 0:LANE], w_s.at[0]),
        (full_w.at[pl.ds(0, 3 * wrow), 0:wide], w_s.at[1]),
        (full_w.at[pl.ds(0, 3 * wrow)], w_s.at[2]),
        (full_w.at[pl.ds(0, width // NC)], w_s.at[3]),
        (ext.at[pl.ds(0, RIM)], w_s.at[4]),
    ):
        pltpu.make_async_copy(ref, ref, sem).wait()
    ref = picked.at[pl.ds(0, slots - CAP)]
    pltpu.make_async_copy(ref, ref, z_s.at[0]).wait()
    ref = home.at[pl.ds(0, slots - CAP)]
    pltpu.make_async_copy(ref, ref, back_s.at[0]).wait()


def per_device(
    branch_in,
    pool_weight,
    group_gain,
    out_weight,
    out_gain,
    ffn_input,
    ffn_gain,
    routes,
    route_weight,
    gate_weight,
    up_weight,
    down_weight,
):
    rows_a, width = branch_in.shape
    rows_b, model = ffn_input.shape
    hid = gate_weight.shape[2]
    top = routes.shape[1]
    slots = NZ * NC * CAP
    wide = NY * LANE
    any_ = pl.BlockSpec(memory_space=pl.ANY)
    vmem = pl.BlockSpec(memory_space=pltpu.VMEM)
    dma = pltpu.SemaphoreType.DMA
    return pl.pallas_call(
        kernel,
        name="mixer_and_experts",
        out_shape=(
            pltpu.VMEM((rows_a, model), BF),
            pltpu.VMEM((rows_b, LANE), BF),
        ),
        in_specs=[any_] * 12,
        out_specs=(vmem, vmem),
        scratch_shapes=[
            pltpu.VMEM(pool_weight.shape, BF),
            pltpu.VMEM((1, width), F32),
            pltpu.VMEM((1, model), F32),
            pltpu.VMEM((1, model), F32),
            pltpu.VMEM((top, rows_b), jnp.int32),
            pltpu.VMEM((top, rows_b), F32),
            pltpu.VMEM((slots, model), BF),
            pltpu.VMEM((width, model), BF),
            pltpu.VMEM((2, model, 2 * hid), BF),
            pltpu.VMEM((2, hid, model), BF),
            pltpu.VMEM((rows_a + RIM, width), BF),
            pltpu.VMEM((rows_a, width), BF),
            pltpu.VMEM((rows_a, model), F32),
            pltpu.VMEM((rows_b, model), BF),
            pltpu.VMEM((slots, rows_b), BF),
            pltpu.VMEM((slots, LANE), BF),
            pltpu.VMEM((slots, model), BF),
            pltpu.VMEM((slots, wide), BF),
            pltpu.VMEM((slots, 2 * wide), BF),
            pltpu.VMEM((slots, wide), BF),
            pltpu.VMEM((slots, LANE), BF),
            pltpu.VMEM((slots, 2 * LANE), BF),
            pltpu.VMEM((slots, LANE), BF),
            pltpu.VMEM((slots, LANE), BF),
            pltpu.VMEM((slots, hid), BF),
            pltpu.VMEM((rows_b, slots), BF),
            pltpu.VMEM((rows_b, slots), BF),
            dma((1,)),
            dma((CHUNKS * 8,)),
            dma((1,)),
            dma((CHUNKS * 8,)),
            dma((5,)),
            dma((14,)),
            dma((1,)),
            dma((CHUNKS,)),
            dma((1,)),
            dma((1,)),
            dma((2,)),
            dma((11,)),
        ],
        compiler_params=pltpu.CompilerParams(collective_id=0, has_side_effects=True),
    )(
        branch_in,
        pool_weight,
        group_gain[None],
        out_weight,
        out_gain[None],
        ffn_input,
        ffn_gain[None],
        routes.T,
        route_weight.T,
        gate_weight,
        up_weight,
        down_weight,
    )


def solution(mesh):
    split = Mesh(mesh.devices.reshape(NZ, NC, NY, NX), AXES)
    in_specs = (
        P(AXES, None),
        P(),
        P(),
        P(None, TP),
        P(),
        P(EP, None),
        P(),
        P(EP, None),
        P(EP, None),
        P(EP, None, TP),
        P(EP, None, TP),
        P(EP, TP, None),
    )
    out_specs = (P(AXES, None), P(EP, TP))
    return jax.shard_map(
        per_device, mesh=split, in_specs=in_specs, out_specs=out_specs, check_vma=False
    )
```

```python
import functools

import jax
import jax.numpy as jnp
from jax import lax
from jax.experimental import pallas as pl
from jax.experimental.pallas import tpu as pltpu
from jax.sharding import Mesh
from jax.sharding import PartitionSpec as P

MESH = pl.DeviceIdType.MESH
AXES = ("z", "c", "y", "x")
EP = ("z", "c")
TP = ("y", "x")

pool_windows = (2, 4, 8, 16)
norm_eps = 1e-06
clamp_limit = 7.0
sigmoid_slope = 1.702

BF = jnp.bfloat16
F32 = jnp.float32

NZ, NC, NY, NX = 16, 2, 4, 4
CAP = 32
LANE = 128
CHUNKS = 8
NEAR = 8
SHARED = {"down": 9, "gate_up": 10}
RIM = 16
WZ = 4
BACK = 1
ORDER = (
    ("ag1", 0), ("ag1", 1), ("ag2", 0, 1), ("ag2", 0, 0), ("ag1", 2), ("w2",), ("ag2", 1, 0), ("ag2", 1, 1),
    ("ag3", 0), ("ag1", 3), ("ag2", 2, 0), ("ag1", 4), ("ag2", 2, 1), ("ag3", 1), ("ag1", 5), ("ag2", 3, 0),
    ("ag4", 0, 0), ("ag4", 0, 1), ("ag1", 6), ("ag2", 3, 1), ("ag1", 7), ("ag4", 1, 0), ("ag3", 2),
    ("ag4", 1, 1), ("pm",), ("ag2", 5, 1), ("ag2", 5, 0), ("ag2", 6, 1), ("ag2", 6, 0), ("ag3", 3), ("w3",),
    ("ag2", 7, 1), ("ag2", 7, 0), ("ag2", 4, 1), ("ag4", 2, 1), ("ag2", 4, 0), ("ag3", 5), ("ag4", 2, 0),
    ("ag4", 3, 1), ("ag4", 3, 0), ("ag3", 6), ("ag3", 7), ("w4",), ("c1", 1), ("ag3", 4), ("ag4", 5, 0),
    ("c1", 0), ("ag4", 5, 1), ("c2", 0), ("c2", 1), ("ag4", 6, 0), ("ag4", 6, 1), ("ag4", 7, 1),
    ("ag4", 7, 0), ("ag4", 4, 0), ("ag4", 4, 1), ("c1", 3), ("c2", 3), ("w5",), ("rs2", 0, 0),
    ("rs2", 0, 1), ("c1", 5), ("c1", 7), ("c1", 6), ("rs2", 3, 0), ("c2", 5), ("rs2", 3, 1), ("c2", 6),
    ("c1", 4), ("c2", 4), ("c2", 7), ("rs3", 0), ("c1", 2), ("rs2", 7, 0), ("rs2", 7, 1), ("rs2", 6, 0),
    ("rs2", 6, 1), ("rs4", 0, 0), ("rs3", 3), ("rs4", 0, 1), ("rs2", 5, 0), ("c2", 2), ("rs2", 4, 1),
    ("rs2", 4, 0), ("rs2", 5, 1), ("rs3", 6), ("rs2", 1, 1), ("rs4", 3, 1), ("rs3", 7), ("rs2", 1, 0),
    ("rs4", 3, 0), ("rs2", 2, 0), ("rs2", 2, 1), ("rs5", 0), ("rs4", 6, 0), ("rs3", 5), ("w6",),
    ("rs4", 6, 1), ("rs3", 4), ("rs4", 7, 1), ("rs4", 7, 0), ("rs3", 1), ("rs5", 3), ("rs3", 2), ("rs5", 6),
    ("rs4", 4, 1), ("rs4", 5, 1), ("rs4", 5, 0), ("rs4", 4, 0), ("rs5", 7), ("rs4", 1, 0), ("rs4", 2, 1),
    ("rs4", 1, 1), ("rs4", 2, 0), ("w7",), ("rs5", 5), ("rs5", 4), ("rs5", 2), ("rs5", 1), ("po",), ("wh",),
)


def dot(a, b):
    return jnp.dot(a, b, preferred_element_type=F32)


def kernel(
    branch,
    pool_w_h,
    group_gain_h,
    out_w,
    out_gain_h,
    ffn_in,
    ffn_gain_h,
    routes_h,
    weight_h,
    gate_w,
    up_w,
    down_w,
    mixer_out,
    expert_out,
    pool_w,
    group_gain,
    out_gain,
    ffn_gain,
    routes_t,
    weight_t,
    full,
    full_w,
    gate_up,
    down,
    ext,
    mixed,
    proj,
    tokens,
    hot,
    picked,
    part,
    rx1,
    rx2,
    sum_x,
    ry1,
    ry2,
    home,
    result,
    hidden,
    w_hi,
    w_lo,
    ag_s,
    ag_r,
    rs_s,
    rs_r,
    w_s,
    w_r,
    z_s,
    z_r,
    back_s,
    back_r,
    own_s,
    load_s,
):
    z, c = lax.axis_index("z"), lax.axis_index("c")
    y, x = lax.axis_index("y"), lax.axis_index("x")
    ep = z * NC + c
    tp = y * NX + x
    tp_p = x * NY + y
    rows_a = branch.shape[0]
    rows_b = ffn_in.shape[0]
    model = ffn_in.shape[1]
    hid = gate_w.shape[2]
    width = branch.shape[1]
    slots = NZ * NC * CAP
    crow = slots // CHUNKS
    half = crow // 2
    per = NZ // CHUNKS
    wide = NY * LANE
    wrow = width // (NC * WZ)

    spot = (ep * NY + y) * NX + x
    total = NZ * NC * NY * NX

    def place(index):
        return (index // (NC * NY * NX), (index // (NY * NX)) % NC, (index // NX) % NY, index % NX)

    after = place((spot + 1) % total)
    before = place((spot + total - 1) % total)
    x_to = ((z, c, y, (x + 1) % NX), (z, c, y, (x + NX - 1) % NX))
    y_to = ((z, c, (y + 1) % NY, x), (z, c, (y + NY - 1) % NY, x))
    z_to = (((z + 1) % NZ, c, y, x), ((z + NZ - 1) % NZ, c, y, x))
    partner = (z, 1 - c, y, x)
    axis_x = (x, x_to)
    axis_y = (y, y_to)

    def order(g):
        return (axis_x, axis_y) if g % 2 == 0 else (axis_y, axis_x)

    def order_back(g):
        return (axis_x, axis_y) if g % 2 == BACK else (axis_y, axis_x)

    def index_of(seat):
        q = seat // per
        return (q if q < NEAR else CHUNKS - 1 + NEAR - q) * per + seat % per

    seat_of = index_of

    def step_z(i):
        return (z + NZ + ((i + 1) // 2) * (2 * (i % 2) - 1)) % NZ

    barrier = pltpu.get_barrier_semaphore()

    def greet(i, carry):
        zz = step_z(i)
        for cc in range(NC):
            pl.semaphore_signal(barrier, inc=1, device_id=(zz, cc, y, x), device_id_type=MESH)
        return carry

    for peer in (*x_to, *y_to, after, before, partner):
        pl.semaphore_signal(barrier, inc=1, device_id=peer, device_id_type=MESH)
    lax.fori_loop(1, NZ, greet, 0)

    loads = {}

    def load(name, src, dst):
        copy = pltpu.make_async_copy(src, dst, load_s.at[SHARED.get(name, len(loads))])
        copy.start()
        if name not in SHARED:
            loads[name] = copy

    own_cols = pl.ds(pl.multiple_of(tp * LANE, LANE), LANE)
    w_rows = pl.ds(pl.multiple_of((c * WZ + z % WZ) * wrow, wrow), wrow)
    load("tokens", ffn_in, tokens)
    load("ffn_gain", ffn_gain_h, ffn_gain)
    load("routes", routes_h, routes_t)
    load("weight", weight_h, weight_t)
    load("out_w", out_w.at[w_rows], full_w.at[w_rows, own_cols])
    load("branch", branch, ext.at[pl.ds(RIM, rows_a)])
    load("pool_w", pool_w_h, pool_w)
    load("group_gain", group_gain_h, group_gain)
    load("out_gain", out_gain_h, out_gain)

    for a in range(NY):
        for b in range(NX):
            here, there = (a * NX + b) * LANE, (b * NY + a) * LANE
            load("down", down_w.at[0, :, pl.ds(here, LANE)], down.at[1, :, pl.ds(there, LANE)])
            for k, w in enumerate((gate_w, up_w)):
                load(
                    "gate_up",
                    w.at[0, pl.ds(here, LANE)],
                    gate_up.at[1, pl.ds(there, LANE), pl.ds(k * hid, hid)],
                )
    load("down", down_w.at[0], down.at[0])
    for k, w in enumerate((gate_w, up_w)):
        load("gate_up", w.at[0], gate_up.at[0, :, pl.ds(k * hid, hid)])

    loads["tokens"].wait()
    acc = jnp.zeros((rows_b, LANE), F32)
    for k in range(model // LANE):
        v = tokens[:, k * LANE : (k + 1) * LANE].astype(F32)
        acc = acc + v * v
    scale = lax.rsqrt(jnp.sum(acc, axis=1, keepdims=True) * (1.0 / model) + norm_eps)
    loads["ffn_gain"].wait()
    normed = (tokens[:, own_cols].astype(F32) * scale * ffn_gain[:, own_cols]).astype(BF)

    loads["routes"].wait()
    loads["weight"].wait()
    experts = NZ * NC
    ids = lax.broadcasted_iota(jnp.int32, (experts, rows_b), 0)
    named = jnp.zeros((experts, rows_b), F32)
    weight = jnp.zeros((experts, rows_b), F32)
    for k in range(routes_t.shape[0]):
        hit = ids == routes_t[k : k + 1, :]
        named = named + jnp.where(hit, 1.0, 0.0)
        weight = weight + jnp.where(hit, weight_t[k : k + 1, :], 0.0)
    earlier = jnp.where(
        lax.broadcasted_iota(jnp.int32, (rows_b, rows_b), 0)
        < lax.broadcasted_iota(jnp.int32, (rows_b, rows_b), 1),
        1.0,
        0.0,
    ).astype(BF)
    place_of = jnp.where(named > 0.5, dot(named.astype(BF), earlier), -1.0)
    slot_ids = lax.broadcasted_iota(jnp.int32, (CAP, rows_b), 0).astype(F32)
    for e in range(experts):
        hot[e * CAP : (e + 1) * CAP, :] = jnp.where(slot_ids == place_of[e : e + 1, :], 1.0, 0.0).astype(BF)
    picked[...] = dot(hot[...], normed).astype(BF)
    loads["out_w"].wait()
    loads["branch"].wait()

    pl.semaphore_wait(barrier, 2 * (NZ - 1) + 7)

    def push(src, dst, sems, index, peer):
        (send, recv), (out, into) = sems, index
        copy = pltpu.make_async_remote_copy(
            src,
            dst,
            send_sem=send.at[out],
            recv_sem=recv.at[into],
            device_id=peer,
            device_id_type=MESH,
        )
        copy.start()
        return copy

    def lanes(which, count):
        return pl.ds(pl.multiple_of(which * count, count), count)

    gather = {}

    def w_block(k, d=None, where=0):
        first, count = (c * WZ + (z + (k if where == 2 else 0) + NZ) % WZ) * wrow, wrow
        if d is not None:
            first, count = first + d * (wrow // 2), wrow // 2
        rows = pl.ds(pl.multiple_of(first, count), count)
        if where == 0:
            return full_w.at[rows, lanes(y * NX + (x + k + NX) % NX, LANE)]
        if where == 1:
            return full_w.at[rows, lanes((y + k + NY) % NY, wide)]
        return full_w.at[rows]

    w_axes = (x_to, y_to, z_to)

    def w_first(where):
        ref = w_block(0, None, where)
        gather["w", where, 0] = [
            push(ref, ref, (w_s, w_r), (where, where * 4 + d), w_axes[where][d]) for d in range(2)
        ]

    def w_second(where):
        out = []
        for d in range(2):
            gather["w", where, 0][d].wait_recv()
            ref = w_block(2 * d - 1, d, where)
            out.append(push(ref, ref, (w_s, w_r), (where, where * 4 + 2 + d), w_axes[where][d]))
        gather["w", where, 1] = out

    def w_third(where):
        for d in range(2):
            gather["w", where, 1][d].wait_recv()

    def w1():
        w_first(0)

    def w2():
        w_second(0)

    def w3():
        w_third(0)
        w_first(1)

    def w4():
        w_second(1)

    def w5():
        w_third(1)
        w_first(2)

    def w6():
        w_second(2)

    def w7():
        w_third(2)
        ref = full_w.at[lanes(c, width // NC)]
        gather["swap"] = push(ref, ref, (w_s, w_r), (3, 12), partner)

    def spread(g, which):
        (a, a_to), (b, b_to) = order(g)
        ref = full.at[pl.ds(g * crow, crow), lanes(b * NX + which % NX, LANE)]
        for d in range(2):
            push(ref, ref, (ag_s, ag_r), (0, g * 8 + 4 + d), b_to[d])

    def ag1(g):
        arrived(g)
        (a, a_to), (b, b_to) = order(g)
        rows = pl.ds(g * crow, crow)
        ref = full.at[rows, lanes(b * NX + a, LANE)]
        gather[g, 0] = [push(ref, ref, (ag_s, ag_r), (0, g * 8 + d), a_to[d]) for d in range(2)]
        spread(g, a)

    def ag2(g, d):
        (a, a_to), (b, b_to) = order(g)
        gather[g, 0][d].wait_recv()
        which = a + NX - 1 + 2 * d
        rows = pl.ds(g * crow + d * half, half)
        ref = full.at[rows, lanes(b * NX + which % NX, LANE)]
        gather[g, 1, d] = push(ref, ref, (ag_s, ag_r), (0, g * 8 + 2 + d), a_to[d])
        spread(g, which)

    def ag3(g):
        (a, a_to), (b, b_to) = order(g)
        for d in range(2):
            gather[g, 1, d].wait_recv()
        spread(g, a + 2)

    def ag4(g, d):
        (a, a_to), (b, b_to) = order(g)
        row = full.at[pl.ds(g * crow, crow), 0:wide]
        pltpu.make_async_copy(row, row, ag_r.at[g * 8 + 4 + d]).wait()
        rows = pl.ds(g * crow + d * half, half)
        ref = full.at[rows, lanes((b + NY - 1 + 2 * d) % NY, wide)]
        gather[g, 3, d] = push(ref, ref, (ag_s, ag_r), (0, g * 8 + 6 + d), b_to[d])

    def seat_ref(seat, cc):
        cols = lanes(tp_p if (seat // per) % 2 else tp, LANE)
        return full.at[lanes(seat * NC + cc, CAP), cols]

    own_pick = pltpu.make_async_copy(picked.at[lanes(ep, CAP)], seat_ref(seat_of(0), c), own_s.at[0])

    def dispatch(zz, cc, seat):
        return pltpu.make_async_remote_copy(
            picked.at[lanes(zz * NC + cc, CAP)],
            seat_ref(seat, c),
            send_sem=z_s.at[0],
            recv_sem=z_r.at[seat // per],
            device_id=(zz, cc, y, x),
            device_id_type=MESH,
        )

    def dispatch_all():
        for seat in range(NZ):
            i = index_of(seat)
            if i == 0:
                own_pick.start()
                dispatch(z, 1 - c, seat).start()
                continue
            back = min(i + 2 * (i % 2) - 1, NZ - 1)
            for cc in range(NC):
                dispatch(step_z(i), cc, seat_of(back)).start()

    def arrived(g):
        own = g == seat_of(0) // per
        ref = full.at[pl.ds(g * crow, crow - CAP if own else crow), 0:LANE]
        pltpu.make_async_copy(ref, ref, z_r.at[g]).wait()
        if own:
            own_pick.wait()

    def pool_mix():
        gather["rim"].wait_recv()
        for name in ("pool_w", "group_gain", "out_gain"):
            loads[name].wait()
        reach = rows_a + RIM
        row = lax.broadcasted_iota(jnp.int32, (rows_a, reach), 0) + RIM
        col = lax.broadcasted_iota(jnp.int32, (rows_a, reach), 1)
        first = jnp.where(spot == 0, RIM, 0)
        age = jnp.where(col < first, reach, row - col)
        position = spot * rows_a + lax.broadcasted_iota(jnp.int32, (rows_a, LANE), 0)
        parts = []
        acc = jnp.zeros((rows_a, LANE), F32)
        for k, window in enumerate(pool_windows):
            cols = slice(k * LANE, (k + 1) * LANE)
            band = jnp.where((age >= 0) & (age < window), 1.0, 0.0).astype(BF)
            summed = dot(band, ext[:, cols])
            count = jnp.minimum(position + 1, window).astype(F32)
            pooled = (summed / count - ext[RIM:, cols].astype(F32)).astype(BF)
            mix = dot(pooled, pool_w[k])
            parts.append(mix)
            acc = acc + mix * mix
        scale = lax.rsqrt(jnp.sum(acc, axis=1, keepdims=True) * (1.0 / width) + norm_eps)
        for k, mix in enumerate(parts):
            cols = slice(k * LANE, (k + 1) * LANE)
            mixed[:, cols] = (mix * scale * group_gain[:, cols]).astype(BF)

    def pool_out():
        gather["swap"].wait_recv()
        acc = jnp.zeros((rows_a, LANE), F32)
        tile = 256
        for n in range(model // tile):
            cols = slice(n * tile, (n + 1) * tile)
            v = dot(mixed[...], full_w[:, cols])
            proj[:, cols] = v
            for k in range(tile // LANE):
                w = v[:, k * LANE : (k + 1) * LANE]
                acc = acc + w * w
        scale = lax.rsqrt(jnp.sum(acc, axis=1, keepdims=True) * (1.0 / model) + norm_eps)
        for n in range(model // tile):
            cols = slice(n * tile, (n + 1) * tile)
            mixer_out[:, cols] = (proj[:, cols] * scale * out_gain[:, cols]).astype(BF)

    def weigh():
        for e in range(0, experts, LANE // CAP):
            rows = []
            for k in range(LANE // CAP):
                h = hot[(e + k) * CAP : (e + k + 1) * CAP, :].astype(F32)
                rows.append(h * weight[e + k : e + k + 1, :])
            turned = jnp.concatenate(rows, axis=0).T
            high = turned.astype(BF)
            cols = slice(e * CAP, e * CAP + LANE)
            w_hi[:, cols] = high
            w_lo[:, cols] = (turned - high.astype(F32)).astype(BF)

    reduce = {}

    def block(which, count):
        return lanes(which % NX, count)

    def down_block(g, k):
        (a, a_to), (b, b_to) = order_back(g)
        rows, cols = pl.ds(g * crow, crow), block(a + 2 + k, wide)
        part[rows, cols] = dot(hidden[rows, :], down[1 if g % 2 == BACK else 0, :, cols]).astype(BF)
        return cols

    def c1(g):
        (a, a_to), (b, b_to) = order_back(g)
        for d in range(2):
            gather[g, 3, d].wait_recv()
        if "weights" not in gather:
            gather["weights"] = True
            for ref, name in ((down, "down"), (gate_up, "gate_up")):
                pltpu.make_async_copy(ref, ref, load_s.at[SHARED[name]]).wait()
        r = g * crow
        both = dot(full[r : r + crow, :], gate_up[g % 2])
        gate = jnp.minimum(both[:, :hid], clamp_limit)
        up = jnp.clip(both[:, hid:], -clamp_limit, clamp_limit)
        hidden[r : r + crow, :] = ((up + 1.0) * gate * jax.nn.sigmoid(sigmoid_slope * gate)).astype(BF)
        cols = down_block(g, 0)
        reduce[g, 0] = [
            push(
                part.at[pl.ds(r + d * half, half), cols],
                rx1.at[pl.ds(r + d * half, half)],
                (rs_s, rs_r),
                (0, g * 8 + d),
                a_to[d],
            )
            for d in range(2)
        ]

    def c2(g):
        for k in range(1, NX):
            down_block(g, k)

    def add(*values):
        out = values[0].astype(F32)
        for v in values[1:]:
            out = out + v.astype(F32)
        return out.astype(BF)

    def rs2(g, d):
        (a, a_to), (b, b_to) = order_back(g)
        r = g * crow
        reduce[g, 0][d].wait_recv()
        cols = block(a + 1 + 2 * d, wide)
        rows = slice(r + d * half, r + d * half + half)
        part[rows, cols] = add(part[rows, cols], rx1[rows, :])
        reduce[g, 1, d] = push(
            part.at[pl.ds(r, crow), cols],
            rx2.at[pl.ds(r, crow), pl.ds(d * wide, wide)],
            (rs_s, rs_r),
            (0, g * 8 + 2 + d),
            a_to[d],
        )

    def rs3(g):
        (a, a_to), (b, b_to) = order_back(g)
        r = g * crow
        for d in range(2):
            reduce[g, 1, d].wait_recv()
        rows = slice(r, r + crow)
        sum_x[rows, :] = add(part[rows, block(a, wide)], rx2[rows, :wide], rx2[rows, wide:])
        cols = block(b + 2, LANE)
        reduce[g, 2] = [
            push(
                sum_x.at[pl.ds(r + d * half, half), cols],
                ry1.at[pl.ds(r + d * half, half)],
                (rs_s, rs_r),
                (0, g * 8 + 4 + d),
                b_to[d],
            )
            for d in range(2)
        ]

    def rs4(g, d):
        (a, a_to), (b, b_to) = order_back(g)
        r = g * crow
        reduce[g, 2][d].wait_recv()
        cols = block(b + 1 + 2 * d, LANE)
        rows = slice(r + d * half, r + d * half + half)
        sum_x[rows, cols] = add(sum_x[rows, cols], ry1[rows, :])
        reduce[g, 3, d] = push(
            sum_x.at[pl.ds(r, crow), cols],
            ry2.at[pl.ds(r, crow), pl.ds(d * LANE, LANE)],
            (rs_s, rs_r),
            (0, g * 8 + 6 + d),
            b_to[d],
        )

    own_rows = lanes(ep, CAP)
    own_back = pltpu.make_async_copy(
        home.at[lanes(seat_of(0) * NC + c, CAP)], result.at[own_rows], own_s.at[1]
    )

    def give_back(seat, cc):
        return pltpu.make_async_remote_copy(
            home.at[lanes(seat * NC + cc, CAP)],
            result.at[own_rows],
            send_sem=back_s.at[0],
            recv_sem=back_r.at[0],
            device_id=(step_z(index_of(seat)), cc, y, x),
            device_id_type=MESH,
        )

    def rs5(g):
        (a, a_to), (b, b_to) = order_back(g)
        r = g * crow
        for d in range(2):
            reduce[g, 3, d].wait_recv()
        rows = slice(r, r + crow)
        home[rows, :] = add(sum_x[rows, block(b, LANE)], ry2[rows, :LANE], ry2[rows, LANE:])
        for seat in range(g * per, (g + 1) * per):
            if index_of(seat) == 0:
                own_back.start()
                give_back(seat, 1 - c).start()
                continue
            for cc in range(NC):
                give_back(seat, cc).start()

    gather["rim"] = push(ext.at[pl.ds(rows_a, RIM)], ext.at[pl.ds(0, RIM)], (w_s, w_r), (4, 13), after)
    w1()
    dispatch_all()

    steps = dict(
        w2=w2, w3=w3, w4=w4, w5=w5, w6=w6, w7=w7, pm=pool_mix, po=pool_out,
        ag1=ag1, ag2=ag2, ag3=ag3, ag4=ag4, c1=c1, c2=c2, rs2=rs2, rs3=rs3, rs4=rs4, rs5=rs5, wh=weigh,
    )
    for name, *where in ORDER:
        steps[name](*where)

    own_back.wait()
    ref = result.at[pl.ds(0, slots - CAP)]
    pltpu.make_async_copy(ref, ref, back_r.at[0]).wait()
    value = dot(w_hi[...], result[...]) + dot(w_lo[...], result[...])
    expert_out[...] = value.astype(BF)
    for ref, sem in (
        (full.at[:, 0 : 3 * LANE + 3 * wide], ag_s.at[0]),
        (part.at[:, 0 : 3 * LANE + 3 * wide], rs_s.at[0]),
        (full_w.at[pl.ds(0, 3 * wrow), 0:LANE], w_s.at[0]),
        (full_w.at[pl.ds(0, 3 * wrow), 0:wide], w_s.at[1]),
        (full_w.at[pl.ds(0, 3 * wrow)], w_s.at[2]),
        (full_w.at[pl.ds(0, width // NC)], w_s.at[3]),
        (ext.at[pl.ds(0, RIM)], w_s.at[4]),
    ):
        pltpu.make_async_copy(ref, ref, sem).wait()
    ref = picked.at[pl.ds(0, slots - CAP)]
    pltpu.make_async_copy(ref, ref, z_s.at[0]).wait()
    ref = home.at[pl.ds(0, slots - CAP)]
    pltpu.make_async_copy(ref, ref, back_s.at[0]).wait()


def per_device(
    branch_in,
    pool_weight,
    group_gain,
    out_weight,
    out_gain,
    ffn_input,
    ffn_gain,
    routes,
    route_weight,
    gate_weight,
    up_weight,
    down_weight,
):
    rows_a, width = branch_in.shape
    rows_b, model = ffn_input.shape
    hid = gate_weight.shape[2]
    top = routes.shape[1]
    slots = NZ * NC * CAP
    wide = NY * LANE
    any_ = pl.BlockSpec(memory_space=pl.ANY)
    vmem = pl.BlockSpec(memory_space=pltpu.VMEM)
    dma = pltpu.SemaphoreType.DMA
    return pl.pallas_call(
        kernel,
        name="mixer_and_experts",
        out_shape=(
            pltpu.VMEM((rows_a, model), BF),
            pltpu.VMEM((rows_b, LANE), BF),
        ),
        in_specs=[any_] * 12,
        out_specs=(vmem, vmem),
        scratch_shapes=[
            pltpu.VMEM(pool_weight.shape, BF),
            pltpu.VMEM((1, width), F32),
            pltpu.VMEM((1, model), F32),
            pltpu.VMEM((1, model), F32),
            pltpu.VMEM((top, rows_b), jnp.int32),
            pltpu.VMEM((top, rows_b), F32),
            pltpu.VMEM((slots, model), BF),
            pltpu.VMEM((width, model), BF),
            pltpu.VMEM((2, model, 2 * hid), BF),
            pltpu.VMEM((2, hid, model), BF),
            pltpu.VMEM((rows_a + RIM, width), BF),
            pltpu.VMEM((rows_a, width), BF),
            pltpu.VMEM((rows_a, model), F32),
            pltpu.VMEM((rows_b, model), BF),
            pltpu.VMEM((slots, rows_b), BF),
            pltpu.VMEM((slots, LANE), BF),
            pltpu.VMEM((slots, model), BF),
            pltpu.VMEM((slots, wide), BF),
            pltpu.VMEM((slots, 2 * wide), BF),
            pltpu.VMEM((slots, wide), BF),
            pltpu.VMEM((slots, LANE), BF),
            pltpu.VMEM((slots, 2 * LANE), BF),
            pltpu.VMEM((slots, LANE), BF),
            pltpu.VMEM((slots, LANE), BF),
            pltpu.VMEM((slots, hid), BF),
            pltpu.VMEM((rows_b, slots), BF),
            pltpu.VMEM((rows_b, slots), BF),
            dma((1,)),
            dma((CHUNKS * 8,)),
            dma((1,)),
            dma((CHUNKS * 8,)),
            dma((5,)),
            dma((14,)),
            dma((1,)),
            dma((CHUNKS,)),
            dma((1,)),
            dma((1,)),
            dma((2,)),
            dma((11,)),
        ],
        compiler_params=pltpu.CompilerParams(collective_id=0, has_side_effects=True),
    )(
        branch_in,
        pool_weight,
        group_gain[None],
        out_weight,
        out_gain[None],
        ffn_input,
        ffn_gain[None],
        routes.T,
        route_weight.T,
        gate_weight,
        up_weight,
        down_weight,
    )


def solution(mesh):
    split = Mesh(mesh.devices.reshape(NZ, NC, NY, NX), AXES)
    in_specs = (
        P(AXES, None),
        P(),
        P(),
        P(None, TP),
        P(),
        P(EP, None),
        P(),
        P(EP, None),
        P(EP, None),
        P(EP, None, TP),
        P(EP, None, TP),
        P(EP, TP, None),
    )
    out_specs = (P(AXES, None), P(EP, TP))
    return jax.shard_map(
        per_device, mesh=split, in_specs=in_specs, out_specs=out_specs, check_vma=False
    )
```
